512 devices in a mesh: sp: 32 (over z, x), tp: 16 (over y, core).
Axes of the slice: x: 4, y: 8, z: 8, core: 2. Of those that a mesh axis runs over, the one named last changes fastest.
Arguments:
- glu_value: bfloat16 [6144, 1024], P('sp', 'tp'), may hold values from -6 to 6
- glu_gate: bfloat16 [6144, 1024], P('sp', 'tp'), may hold values from -6 to 6
- doc_ids: int32 [6144], P('sp'), may hold values from 0 to 15, never falling along the last dimension, each value on 1 to 768 neighbouring positions
- conv_kernel: bfloat16 [31, 1024], P(None, 'tp')
- conv_gain: float32 [1024], P('tp'), may hold values from 0.1 to 1.9
- out_weight: bfloat16 [1024, 2048], P('tp'), may hold values from -0.1875 to 0.1875
- residual: bfloat16 [6144, 2048], P('sp'), may hold values from -6 to 6
- mix_gain: float32 [2048], replicated, may hold values from 0.1 to 1.9
- routes: int32 [6144, 2], P('sp'), may hold values from 0 to 31, all different within a row; in each aligned block of 192 rows (0 to 191, 192 to 383, ...) at most 24 rows name the same one
- route_weights: float32 [6144, 2], P('sp'), may hold values from 0.2 to 1
- expert_gate: bfloat16 [32, 2048, 5120], P('sp', None, 'tp'), may hold values from -0.125 to 0.125
- expert_up: bfloat16 [32, 2048, 5120], P('sp', None, 'tp'), may hold values from -0.125 to 0.125
- expert_down: bfloat16 [32, 5120, 2048], P('sp', 'tp')
- final_gain: float32 [2048], P('tp'), may hold values from 0.1 to 1.9
Outputs:
- block_out: bfloat16 [6144, 2048], P('sp', 'tp')
The draws below stay inside these ranges and needn't reach their ends.
Inputs may be any that keep to these rules, and one draw needn't show every extreme that they name: `routes`: each row names two different experts. In each aligned block of 192 rows no expert is named by more than 24 rows, and in every draw some block has an expert named by exactly 24 rows. `doc_ids`: document numbers never fall along the sequence.
All inputs are finite; a program needn't handle non-finite values.
Results may differ from the reference program's by a relative error of at most 0.022.
Values may be sent and summed in bfloat16 or wider, within the bound.
No kernel may reach another device: no remote copies, remote signals or barrier semaphores. Data moves between devices by JAX's collectives and lax.ppermute only.
A program may use at most 64 MiB of HBM per device.

```python
import math
import jax
import jax.numpy as jnp
import numpy as np
from jax import lax

D = 2048
C = 1024
FF = 5120
WIDTH = 31
TOK = 192
EXPERTS = 32
TOKENS = 6144
CAP = 24
DOCS = 16
DOC_MOST = 768
N_SP = 32
N_TP = 16


def draw_conv_kernel(key, part):
    base_draw = jax.random.normal(key, (WIDTH, C), jnp.float32)
    ramp_scale = jnp.exp(jnp.log(4.0) * jnp.arange(C, dtype=jnp.float32) / C)[None, :]
    return (base_draw * ramp_scale * WIDTH ** (-0.5)).astype(jnp.bfloat16)


def draw_expert_down(key, part):
    ramp_scale = jnp.exp(jnp.log(4.0) * (jnp.arange(D, dtype=jnp.float32) / D - 0.5))[None, None, :]
    base_draw = jax.random.normal(key, (EXPERTS, FF, D), jnp.float32)
    return (base_draw * ramp_scale * FF ** (-0.5)).astype(jnp.bfloat16)


def steps_of(stream_key, dims, cuts, least, top_value):
    level = 1.0
    for dim, shards_of in cuts:
        steps = jax.random.uniform(jax.random.fold_in(jax.random.fold_in(stream_key, 6), dim), (shards_of,), jnp.float32, least / len(cuts), top_value / len(cuts))
        level = level * jnp.repeat(jnp.exp(steps), dims[dim] // shards_of).reshape((-1,) + (1,) * (len(dims) - 1 - dim))
    return level


def profile(amount, total, reach, skew):
    weights = [(1 << 20) // math.isqrt(grade ** skew) + 1 for grade in range(2, amount + 1)]
    surplus, counts = total - reach - (amount - 1), [1] * (amount - 1)
    while surplus > 0:
        movable = [i for i in range(amount - 1) if counts[i] < reach]
        pool, left = sum([weights[i] for i in movable]), surplus
        for i in movable:
            addition = min(reach - counts[i], max(1, left * weights[i] // pool), surplus)
            counts[i] = counts[i] + addition
            surplus = surplus - addition
    return np.array([reach] + counts)


def uneven(key, number_of, total, most, skew):
    if number_of == 2:
        one = jax.random.randint(key, (), max(1, total - most), min(most, total - 1) + 1)
        return jnp.stack([one, total - one])
    sizes = jnp.asarray(profile(number_of, total, most, skew), jnp.int32)
    pairs = (number_of - 1) // 2
    giver, receiver = sizes[1:1 + 2 * pairs:2], sizes[2:2 + 2 * pairs:2]
    slack = jnp.minimum(giver - 1, most - receiver)
    shifted = jax.random.randint(jax.random.fold_in(key, 1), (pairs,), 0, 1 << 20) % (slack + 1)
    sizes = sizes.at[1:1 + 2 * pairs:2].set(giver - shifted).at[2:2 + 2 * pairs:2].set(receiver + shifted)
    return sizes[jax.random.permutation(jax.random.fold_in(key, 2), number_of)]


def shared_out(rng, own, number, rows, number_of, top, limit, lean):
    sequence = jax.random.permutation(rng, number_of)
    heavy_load, common = portions_of(number_of, rows * top, limit, lean, True), portions_of(number_of, rows * top, limit, lean, False)
    places = jnp.arange(number_of)

    def named(lengths, rotation):
        used = int((lengths > 0).sum())
        fixed = max(1, used // 4)
        moved = fixed + (places - fixed + rotation * (used - fixed)) % max(1, number_of - fixed)
        return jnp.zeros((number_of,), jnp.int32).at[sequence[jnp.where(places < fixed, places, moved)]].set(jnp.asarray(lengths, jnp.int32))

    lengths = jnp.where(number % 4 == 0, named(heavy_load, number // 4), named(common, number - number // 4 - 1))
    mixed = jax.random.permutation(jax.random.fold_in(own, 3), number_of)
    giver, sink = mixed[0:number_of // 2 * 2:2], mixed[1:number_of // 2 * 2:2]
    room = jnp.minimum(lengths[giver] - 1, limit - lengths[sink]) // 2
    room = jnp.where((giver == sequence[0]) | (sink == sequence[0]) | (lengths[sink] == 0), 0, jnp.maximum(room, 0))
    moved = jax.random.randint(jax.random.fold_in(own, 4), (number_of // 2,), 0, 1 << 20) % (room + 1)
    lengths = lengths.at[giver].add(-moved).at[sink].add(moved)
    members = jnp.searchsorted(jnp.cumsum(lengths), jnp.arange(rows * top), side="right").astype(jnp.int32)
    grid = members.reshape(top, rows).T
    grid = grid[jax.random.permutation(jax.random.fold_in(own, 1), rows)]
    rotation = jax.random.randint(jax.random.fold_in(own, 2), (rows, 1), 0, top)
    return jnp.take_along_axis(grid, (jnp.arange(top)[None, :] + rotation) % top, axis=1)


def portions_of(amount, total, most, slope, full):
    loads = [(1 << 20) // math.isqrt(grade ** slope) + 1 for grade in range(1, amount + 1)]
    largest = most if full else min(most, max(-(-total // amount), total * loads[0] // sum(loads)))
    least = 1 if total - largest >= amount - 1 else 0
    counts, spare = [largest] + [least] * (amount - 1), total - largest - least * (amount - 1)
    while spare > 0:
        movable = [i for i in range(1, amount) if counts[i] < largest] or [i for i in range(1, amount) if counts[i] < most]
        pool, budget = sum([loads[i] for i in movable]), spare
        for i in movable:
            more = min(most - counts[i], max(1, budget * loads[i] // pool), spare)
            counts[i] = counts[i] + more
            spare = spare - more
    return np.array(counts)


def bell_draw(key, extent, spread, bound, split=(), kind=jnp.bfloat16):
    drawn = jax.random.normal(key, extent, jnp.float32) * spread
    if len(split) > 0:
        drawn = steps_of(key, extent, split, -0.22, 0.18) * drawn
    return jnp.clip(drawn, min=-bound, max=bound).astype(kind)


def setup_inputs(seed: int = 0) -> dict:
    splits = jax.random.split(jax.random.key(seed), 15)
    glu_value = bell_draw(splits[0], (TOKENS, C), 1.0, 6.0, ((0, 32), (1, 16)))
    glu_gate = bell_draw(splits[1], (TOKENS, C), 1.0, 6.0, ((0, 32), (1, 16)))
    doc_ids = jnp.searchsorted(jnp.cumsum(uneven(splits[2], DOCS, TOKENS, DOC_MOST, 1)), jnp.arange(TOKENS), side="right").astype(jnp.int32)
    conv_kernel = draw_conv_kernel(jax.random.fold_in(splits[14], 71), 0)
    conv_gain = jnp.clip(1.0 + 0.18 * jax.random.normal(splits[4], (C,), jnp.float32), 0.1, 1.9)
    out_weight = bell_draw(splits[5], (C, D), C ** -0.5, 0.1875, ((0, 16),))
    residual = bell_draw(splits[6], (TOKENS, D), 1.0, 6.0, ((0, 32),))
    mix_gain = jnp.clip(1.0 + 0.18 * jax.random.normal(splits[7], (D,), jnp.float32), 0.1, 1.9)
    routes_keys = jax.random.split(jax.random.fold_in(splits[8], 1), TOKENS // TOK)
    routes_turns = jax.random.permutation(jax.random.fold_in(splits[8], 3), TOKENS // TOK)
    routes = jax.vmap(lambda own, number: shared_out(jax.random.fold_in(splits[8], 2), own, number, TOK, EXPERTS, 2, CAP, 2))(routes_keys, routes_turns).reshape((TOKENS, 2))
    route_weights = jnp.clip(0.2 + 0.8 * jax.random.uniform(splits[9], (TOKENS, 2), jnp.float32) ** steps_of(splits[9], (TOKENS, 2), ((0, 32),), -0.2, 0.2), 0.2, 1.0)
    expert_gate = bell_draw(splits[10], (EXPERTS, D, FF), D ** -0.5, 0.125, ((0, 32), (2, 16)))
    expert_up = bell_draw(splits[11], (EXPERTS, D, FF), D ** -0.5, 0.125, ((0, 32), (2, 16)))
    expert_down = draw_expert_down(jax.random.fold_in(splits[14], 71), 0)
    final_gain = jnp.clip(1.0 + 0.18 * jax.random.normal(splits[13], (D,), jnp.float32), 0.1, 1.9)
    return {"glu_value": glu_value, "glu_gate": glu_gate, "doc_ids": doc_ids, "conv_kernel": conv_kernel, "conv_gain": conv_gain, "out_weight": out_weight, "residual": residual, "mix_gain": mix_gain, "routes": routes, "route_weights": route_weights, "expert_gate": expert_gate, "expert_up": expert_up, "expert_down": expert_down, "final_gain": final_gain}


residual_alpha = 1.41421356
norm_eps = 1e-05

def scaled_norm(pre_norm, gain):
    row_mean = lax.optimization_barrier(jnp.mean(pre_norm, -1, keepdims=True))
    row_var = lax.optimization_barrier(jnp.mean(pre_norm * pre_norm, -1, keepdims=True)) - row_mean * row_mean
    return (pre_norm - row_mean) * lax.rsqrt(row_var + norm_eps) * gain

def reference(glu_value, glu_gate, doc_ids, conv_kernel, conv_gain, out_weight, residual, mix_gain, routes, route_weights, expert_gate, expert_up, expert_down, final_gain):
    seq_len = glu_value.shape[0]
    gated_rows = (glu_value.astype(jnp.float32) * jax.nn.sigmoid(glu_gate.astype(jnp.float32))).astype(jnp.bfloat16)
    gated_wide = gated_rows.astype(jnp.float32)
    kernel = conv_kernel.astype(jnp.float32)
    filtered = jnp.zeros(gated_wide.shape, jnp.float32)
    for shift_by in range(WIDTH):
        moved_rows = jnp.pad(gated_wide, ((shift_by, 0), (0, 0)))[:seq_len]
        moved_ids = jnp.pad(doc_ids, (shift_by, 0), constant_values=-1)[:seq_len]
        same_doc = (moved_ids == doc_ids)[:, None]
        filtered = filtered + jnp.where(same_doc, moved_rows, 0.0) * kernel[shift_by]
    conv_out = jax.nn.silu(scaled_norm(filtered, conv_gain.astype(jnp.float32))).astype(jnp.bfloat16)
    width_block = C // N_TP
    mix_total = jnp.zeros((seq_len, D), jnp.float32)
    for block_at in range(N_TP):
        columns = conv_out[:, block_at * width_block:(block_at + 1) * width_block]
        weights = out_weight[block_at * width_block:(block_at + 1) * width_block]
        mix_total = mix_total + jnp.dot(columns, weights, preferred_element_type=jnp.float32).astype(jnp.bfloat16).astype(jnp.float32)
    mixed_rows = scaled_norm(residual_alpha * residual.astype(jnp.float32) + mix_total, mix_gain.astype(jnp.float32)).astype(jnp.bfloat16)
    chosen = routes.reshape(N_SP, TOK * 2)
    member = (chosen[:, :, None] == jnp.arange(EXPERTS, dtype=jnp.int32)[None, None, :]).astype(jnp.int32)
    earlier = jnp.cumsum(member, 1) - member
    rank_in = lax.optimization_barrier(jnp.sum(earlier * member, -1))
    group_at = jnp.arange(N_SP, dtype=jnp.int32)[:, None]
    row_at = (group_at * CAP + rank_in).reshape(-1).astype(jnp.int32)
    expert_at = chosen.reshape(-1).astype(jnp.int32)
    token_at = jnp.repeat(jnp.arange(seq_len, dtype=jnp.int32), 2)
    expert_inbox = jnp.zeros((EXPERTS, N_SP * CAP, D), jnp.bfloat16).at[expert_at, row_at].set(mixed_rows[token_at])
    hidden_block = FF // N_TP

    def run_expert(packed):
        in_rows, w_gate, w_up, w_down = packed
        gate_proj = jnp.dot(in_rows, w_gate, preferred_element_type=jnp.float32)
        up_proj = jnp.dot(in_rows, w_up, preferred_element_type=jnp.float32)
        hidden = (jax.nn.silu(gate_proj) * up_proj).astype(jnp.bfloat16)
        running = jnp.zeros((in_rows.shape[0], D), jnp.float32)
        for block_at in range(N_TP):
            piece_out = jnp.dot(hidden[:, block_at * hidden_block:(block_at + 1) * hidden_block], w_down[block_at * hidden_block:(block_at + 1) * hidden_block], preferred_element_type=jnp.float32)
            running = running + piece_out.astype(jnp.bfloat16).astype(jnp.float32)
        return running.astype(jnp.bfloat16)
    expert_outbox = lax.map(run_expert, (expert_inbox, expert_gate, expert_up, expert_down))
    picked = expert_outbox[expert_at, row_at].astype(jnp.float32).reshape(seq_len, 2, D)
    moe_sum = lax.optimization_barrier(jnp.sum(route_weights[:, :, None] * picked, 1))
    pre_norm = residual_alpha * mixed_rows.astype(jnp.float32) + moe_sum
    return scaled_norm(pre_norm, final_gain.astype(jnp.float32)).astype(jnp.bfloat16)
```

```python
import jax
import jax.numpy as jnp
from jax import lax
from jax.sharding import Mesh
from jax.sharding import PartitionSpec as P

TP = ("y", "c")

residual_alpha = 1.41421356
norm_eps = 1e-05
row_scale = 64.0


def from_behind(value, axis, by):
    peers = lax.axis_size(axis)
    pairs = [(i, i + by) for i in range(peers) if 0 <= i + by < peers]
    return lax.ppermute(value, axis, pairs)


def swap(value, axis):
    return lax.ppermute(value, axis, [(0, 1), (1, 0)])


def summed_over(value, axis, peers):
    copies = jnp.broadcast_to(value[None], (peers, *value.shape))
    return jnp.sum(lax.all_to_all(copies, axis, 0, 0, tiled=True), axis=0)


def local(
    glu_value,
    glu_gate,
    doc_ids,
    conv_kernel,
    conv_gain,
    out_weight,
    residual,
    mix_gain,
    routes,
    route_weights,
    expert_gate,
    expert_up,
    expert_down,
    final_gain,
):
    f32, bf16 = jnp.float32, jnp.bfloat16
    n_sp, n_y, n_c = lax.axis_size("sp"), lax.axis_size("y"), lax.axis_size("c")
    n_tp = n_y * n_c
    at_c = lax.axis_index("c")
    at_tp = lax.axis_index(TP)
    tok_rows, own_ch = glu_value.shape
    rim_len = conv_kernel.shape[0] - 1
    channels = own_ch * n_tp
    features = residual.shape[1]
    feat_block = features // n_tp

    gated_rows = (glu_value.astype(f32) * jax.nn.sigmoid(glu_gate.astype(f32))).astype(bf16)
    rim_rows, rim_ids = from_behind(
        (gated_rows[tok_rows - rim_len :], doc_ids[tok_rows - rim_len :]), "sp", 1
    )
    packed = jnp.concatenate(
        [rim_rows.astype(f32), gated_rows.astype(f32), conv_kernel.astype(f32), conv_gain[None]], 0
    )
    packed = lax.all_gather(packed, "c", axis=1, tiled=True)
    extended = packed[: rim_len + tok_rows]
    kernel = packed[rim_len + tok_rows : 2 * rim_len + tok_rows + 1]
    gain = packed[2 * rim_len + tok_rows + 1]
    ext_ids = jnp.concatenate([rim_ids, doc_ids], 0)
    filtered = jnp.zeros((tok_rows, n_c * own_ch), f32)
    for shift_by in range(rim_len + 1):
        begin_at = rim_len - shift_by
        same_doc = (ext_ids[begin_at : begin_at + tok_rows] == doc_ids)[:, None]
        filtered = (
            filtered
            + jnp.where(same_doc, extended[begin_at : begin_at + tok_rows], 0.0) * kernel[shift_by]
        )
    stats = summed_over(
        jnp.concatenate([jnp.sum(filtered, 1), jnp.sum(filtered * filtered, 1)]).reshape(-1, 128),
        "y",
        n_y,
    ).reshape(2, tok_rows)
    row_mean = stats[0][:, None] / channels
    row_var = stats[1][:, None] / channels - row_mean * row_mean
    conv_out = jax.nn.silu((filtered - row_mean) * lax.rsqrt(row_var + norm_eps) * gain).astype(bf16)

    weight_parts = out_weight.reshape(own_ch, n_y, n_c, feat_block).transpose(2, 0, 1, 3)
    weight_half = lax.all_to_all(weight_parts, "c", 0, 0, tiled=True)
    weight_half = weight_half.reshape(n_c * own_ch, n_y, feat_block)
    mix_parts = jnp.einsum("tk,kyf->ytf", conv_out, weight_half, preferred_element_type=f32)
    mix_parts = lax.all_to_all(mix_parts.astype(bf16), "y", 0, 0, tiled=True)
    own_residual = lax.dynamic_slice_in_dim(residual, at_tp * feat_block, feat_block, 1)
    own_z = residual_alpha * own_residual.astype(f32) + jnp.sum(mix_parts.astype(f32), 0)

    experts = expert_gate.shape[0] * n_sp
    capacity = 4 * tok_rows // experts
    chosen = routes.reshape(-1)
    member = (chosen[:, None] == jnp.arange(experts, dtype=jnp.int32)[None, :]).astype(jnp.int32)
    earlier = jnp.cumsum(member, 0) - member
    slot_index = (chosen * capacity + jnp.sum(earlier * member, 1)).reshape(tok_rows, 2)
    slots = jnp.arange(experts * capacity, dtype=jnp.int32)
    dispatch_table = jnp.any(slots[:, None, None] == slot_index[None], -1).astype(bf16)

    outgoing = jnp.dot(dispatch_table, own_z.astype(bf16), preferred_element_type=f32)
    outgoing = (outgoing * row_scale).astype(jnp.float16).reshape(experts, capacity, feat_block)
    arrived = lax.all_to_all(outgoing, "sp", 0, 0, tiled=True)
    rows = n_sp * capacity
    gathered = lax.all_gather(arrived.reshape(rows, feat_block), TP, axis=0, tiled=False)

    wide = gathered.astype(f32)
    in_mean = jnp.sum(wide, (0, 2)) * (1.0 / (row_scale * features))
    in_square = jnp.sum(wide * wide, (0, 2)) * (1.0 / (row_scale * row_scale * features))
    in_rstd = lax.rsqrt(in_square - in_mean * in_mean + norm_eps)
    in_rows = (
        (wide * (1.0 / row_scale) - in_mean[None, :, None])
        * in_rstd[None, :, None]
        * mix_gain.reshape(n_tp, 1, feat_block)
    ).astype(bf16)
    in_rows = in_rows.transpose(1, 0, 2).reshape(rows, features)
    gate_proj = jnp.dot(in_rows, expert_gate[0], preferred_element_type=f32)
    up_proj = jnp.dot(in_rows, expert_up[0], preferred_element_type=f32)
    hidden = (jax.nn.silu(gate_proj) * up_proj).astype(bf16)

    down_parts = expert_down[0].reshape(-1, n_y, n_c, feat_block)
    down_mine = lax.dynamic_index_in_dim(down_parts, at_c, 2, keepdims=False)
    down_else = swap(lax.dynamic_index_in_dim(down_parts, 1 - at_c, 2, keepdims=False), "c")
    hidden_else = swap(hidden, "c")
    hidden_both = jnp.concatenate([hidden, hidden_else], 1)
    down_both = jnp.concatenate([down_mine, down_else], 0)
    parts = jnp.einsum(
        "sik,kyf->syif",
        hidden_both.reshape(n_sp, capacity, -1),
        down_both,
        preferred_element_type=f32,
    ).astype(bf16)
    parts = parts.reshape(n_sp * n_y, capacity, feat_block)
    returned = lax.all_to_all(parts, ("sp", "y"), 0, 0, tiled=True)
    returned = returned.reshape(experts, n_y, capacity, feat_block)
    expert_out = jnp.sum(returned.astype(f32), 1).astype(bf16).reshape(experts * capacity, feat_block)
    first = (slot_index[:, :1] == slots[None, :]).astype(bf16)
    second = (slot_index[:, 1:] == slots[None, :]).astype(bf16)
    moe_sum = route_weights[:, :1] * jnp.dot(
        first, expert_out, preferred_element_type=f32
    ) + route_weights[:, 1:] * jnp.dot(second, expert_out, preferred_element_type=f32)

    own_gain = lax.dynamic_slice_in_dim(mix_gain, at_tp * feat_block, feat_block, 0)[None]
    z_gain = own_z * own_gain
    sums = jnp.stack(
        [
            jnp.sum(own_z, 1),
            jnp.sum(own_z * own_z, 1),
            jnp.sum(z_gain, 1),
            jnp.sum(z_gain * z_gain, 1),
            jnp.sum(z_gain * own_gain, 1),
            jnp.sum(z_gain * moe_sum, 1),
            jnp.sum(own_gain * moe_sum, 1),
            jnp.sum(moe_sum, 1),
            jnp.sum(moe_sum * moe_sum, 1),
            jnp.zeros_like(moe_sum[:, 0]),
        ]
    )
    sums = summed_over(sums.reshape(-1, 128), TP, n_tp).reshape(10, tok_rows)
    z_mean = sums[0] / features
    z_rstd = lax.rsqrt(sums[1] / features - z_mean * z_mean + norm_eps)
    ar = residual_alpha * z_rstd
    fin_sum = ar * (sums[2] - z_mean * jnp.sum(mix_gain)) + sums[7]
    fin_square = (
        ar * ar * (sums[3] - 2.0 * z_mean * sums[4] + z_mean * z_mean * jnp.sum(mix_gain * mix_gain))
        + 2.0 * ar * (sums[5] - z_mean * sums[6])
        + sums[8]
    )
    fin_mean = fin_sum / features
    fin_rstd = lax.rsqrt(fin_square / features - fin_mean * fin_mean + norm_eps)
    pre_norm = ar[:, None] * (own_z - z_mean[:, None]) * own_gain + moe_sum
    return ((pre_norm - fin_mean[:, None]) * fin_rstd[:, None] * final_gain).astype(bf16)


def solution(mesh):
    finer = Mesh(mesh.devices.reshape(mesh.shape["sp"], 8, 2), ("sp", "y", "c"))
    placed = (
        P("sp", TP),
        P("sp", TP),
        P("sp"),
        P(None, TP),
        P(TP),
        P(TP, None),
        P("sp", None),
        P(),
        P("sp", None),
        P("sp", None),
        P("sp", None, TP),
        P("sp", None, TP),
        P("sp", TP, None),
        P(TP),
    )
    return jax.shard_map(local, mesh=finer, in_specs=placed, out_specs=P("sp", TP), check_vma=False)
```

```python
import functools

import jax
import jax.numpy as jnp
from jax import lax
from jax.experimental import pallas as pl
from jax.experimental.pallas import tpu as pltpu
from jax.sharding import Mesh
from jax.sharding import PartitionSpec as P

TP = ("y", "c")

residual_alpha = 1.41421356
norm_eps = 1e-05
row_scale = 64.0


def from_behind(value, axis, by):
    peers = lax.axis_size(axis)
    pairs = [(i, i + by) for i in range(peers) if 0 <= i + by < peers]
    return lax.ppermute(value, axis, pairs)


def swap(value, axis):
    return lax.ppermute(value, axis, [(0, 1), (1, 0)])


def summed_over(value, axis, peers):
    copies = jnp.broadcast_to(value[None], (peers, *value.shape))
    return jnp.sum(lax.all_to_all(copies, axis, 0, 0, tiled=True), axis=0)


def conv_body(packed_ref, ids_ref, filtered_ref, sums_ref, *, lags, tok_rows):
    packed = packed_ref[...]
    ids = ids_ref[...]
    total = jnp.zeros((packed.shape[0], tok_rows), jnp.float32)
    for lag in range(lags):
        rows = packed if lag == 0 else pltpu.roll(packed, lag, 1)
        other = ids if lag == 0 else pltpu.roll(ids, lag, 1)
        same_doc = other[:1, :tok_rows] == ids[:1, :tok_rows]
        tap = packed[:, tok_rows + lag : tok_rows + lag + 1]
        total = total + jnp.where(same_doc, rows[:, :tok_rows], 0.0) * tap
    filtered_ref[...] = total
    sums = jnp.concatenate(
        [jnp.sum(total, 0, keepdims=True), jnp.sum(total * total, 0, keepdims=True)], 0
    )
    sums_ref[...] = jnp.broadcast_to(sums[None], sums_ref.shape)


def mix_body(at_ref, filtered_ref, sums_ref, packed_ref, mine_ref, else_ref, out_ref, *, gain_at, channels):
    first = at_ref[0] == 0
    peers, tok_rows, block = out_ref.shape
    sums = jnp.sum(sums_ref[...], 0)
    row_mean = sums[:1] / channels
    row_var = sums[1:] / channels - row_mean * row_mean
    gain = packed_ref[:, gain_at : gain_at + 1]
    normed = (filtered_ref[...] - row_mean) * lax.rsqrt(row_var + norm_eps) * gain
    conv_out = (normed / (1.0 + jnp.exp(-normed))).T.astype(jnp.bfloat16)
    for peer in range(0, peers, 2):
        columns = []
        for step in range(2):
            at = pl.multiple_of((2 * (peer + step) + at_ref[0]) * block, block)
            mine, other = mine_ref[:, pl.ds(at, block)], else_ref[:, pl.ds(at, block)]
            columns.append(
                jnp.concatenate([jnp.where(first, mine, other), jnp.where(first, other, mine)], 0)
            )
        part = jnp.dot(
            conv_out, jnp.concatenate(columns, 1), preferred_element_type=jnp.float32
        ).astype(jnp.bfloat16)
        out_ref[peer] = part[:, :block]
        out_ref[peer + 1] = part[:, block:]


def down_body(at_ref, mine_ref, else_ref, down_mine_ref, down_else_ref, out_ref):
    n_sp, peers, capacity, block = out_ref.shape
    hidden = jnp.concatenate([mine_ref[...], else_ref[...]], 0)
    for peer in range(0, peers, 2):
        columns = []
        for step in range(2):
            at = pl.multiple_of((2 * (peer + step) + at_ref[0]) * block, block)
            columns.append(
                jnp.concatenate([down_mine_ref[:, pl.ds(at, block)], down_else_ref[:, pl.ds(at, block)]], 0)
            )
        part = lax.dot_general(
            hidden,
            jnp.concatenate(columns, 1),
            (((0,), (0,)), ((), ())),
            preferred_element_type=jnp.float32,
        ).astype(jnp.bfloat16)
        out_ref[:, peer] = part[:, :block].reshape(n_sp, capacity, block)
        out_ref[:, peer + 1] = part[:, block:].reshape(n_sp, capacity, block)


def whole(memory=None):
    return pl.BlockSpec(memory_space=memory or pltpu.VMEM)


def local(
    glu_value,
    glu_gate,
    doc_ids,
    conv_kernel,
    conv_gain,
    out_weight,
    residual,
    mix_gain,
    routes,
    route_weights,
    expert_gate,
    expert_up,
    expert_down,
    final_gain,
):
    f32, bf16 = jnp.float32, jnp.bfloat16
    n_sp, n_y, n_c = lax.axis_size("sp"), lax.axis_size("y"), lax.axis_size("c")
    n_tp = n_y * n_c
    at_core = lax.axis_index("c").astype(jnp.int32).reshape(1)
    at_tp = lax.axis_index(TP)
    tok_rows, own_ch = glu_value.shape
    lags = conv_kernel.shape[0]
    rim_len = lags - 1
    channels = own_ch * n_tp
    features = residual.shape[1]
    feat_block = features // n_tp

    value, gate = glu_value.T.astype(f32), glu_gate.T.astype(f32)
    gated = (value * jax.nn.sigmoid(gate)).astype(bf16)
    ids = doc_ids.astype(f32)[None]
    rim = jnp.concatenate([gated[:, tok_rows - rim_len :], ids[:, tok_rows - rim_len :].astype(bf16)], 0)
    rim = from_behind(rim, "sp", 1).astype(f32)
    lanes = 256
    blank = lanes - tok_rows - lags - 1 - rim_len
    packed = jnp.concatenate(
        [
            gated.astype(f32),
            conv_kernel.T.astype(f32),
            conv_gain[:, None],
            jnp.zeros((own_ch, blank), f32),
            rim[:own_ch],
        ],
        1,
    )
    packed = lax.all_gather(packed, "c", axis=0, tiled=True)
    packed_ids = jnp.concatenate(
        [ids, jnp.zeros((1, lanes - tok_rows - rim_len), f32), rim[own_ch:]], 1
    )
    packed_ids = jnp.broadcast_to(packed_ids, (8, lanes))
    filtered, sums = pl.pallas_call(
        functools.partial(conv_body, lags=lags, tok_rows=tok_rows),
        out_shape=(
            jax.ShapeDtypeStruct((n_c * own_ch, tok_rows), f32),
            jax.ShapeDtypeStruct((n_y, 2, tok_rows), f32),
        ),
        in_specs=[whole()] * 2,
        out_specs=(whole(), whole()),
        name="conv",
    )(packed, packed_ids)
    sums = lax.all_to_all(sums, "y", 0, 0, tiled=True)
    weight_else = swap(out_weight, "c")
    mix_parts = pl.pallas_call(
        functools.partial(mix_body, gain_at=tok_rows + lags, channels=channels),
        out_shape=jax.ShapeDtypeStruct((n_y, tok_rows, feat_block), bf16),
        in_specs=[whole(pltpu.SMEM)] + [whole()] * 5,
        out_specs=whole(),
        name="mix",
    )(at_core, filtered, sums, packed, out_weight, weight_else)
    mix_parts = lax.all_to_all(mix_parts, "y", 0, 0, tiled=True)
    own_residual = lax.dynamic_slice_in_dim(residual, at_tp * feat_block, feat_block, 1)
    own_z = residual_alpha * own_residual.astype(f32) + jnp.sum(mix_parts.astype(f32), 0)

    experts = expert_gate.shape[0] * n_sp
    capacity = 4 * tok_rows // experts
    chosen = routes.reshape(-1)
    member = (chosen[:, None] == jnp.arange(experts, dtype=jnp.int32)[None, :]).astype(jnp.int32)
    earlier = jnp.cumsum(member, 0) - member
    slot_index = (chosen * capacity + jnp.sum(earlier * member, 1)).reshape(tok_rows, 2)
    slots = jnp.arange(experts * capacity, dtype=jnp.int32)
    dispatch_table = jnp.any(slots[:, None, None] == slot_index[None], -1).astype(bf16)

    outgoing = jnp.dot(dispatch_table, own_z.astype(bf16), preferred_element_type=f32)
    outgoing = (outgoing * row_scale).astype(jnp.float16).reshape(experts, capacity, feat_block)
    arrived = lax.all_to_all(outgoing, "sp", 0, 0, tiled=True)
    rows = n_sp * capacity
    gathered = lax.all_gather(arrived.reshape(rows, feat_block).T, TP, axis=0, tiled=True)

    wide = gathered.astype(f32)
    in_mean = jnp.sum(wide, 0) * (1.0 / (row_scale * features))
    in_square = jnp.sum(wide * wide, 0) * (1.0 / (row_scale * row_scale * features))
    in_rstd = lax.rsqrt(in_square - in_mean * in_mean + norm_eps)
    in_rows = (
        (wide * (1.0 / row_scale) - in_mean[None]) * in_rstd[None] * mix_gain[:, None]
    ).astype(bf16)
    gate_proj = jnp.einsum("kf,kr->fr", expert_gate[0], in_rows, preferred_element_type=f32)
    up_proj = jnp.einsum("kf,kr->fr", expert_up[0], in_rows, preferred_element_type=f32)
    hidden = (jax.nn.silu(gate_proj) * up_proj).astype(bf16)

    w_down = expert_down[0]
    parts = pl.pallas_call(
        down_body,
        out_shape=jax.ShapeDtypeStruct((n_sp, n_y, capacity, feat_block), bf16),
        in_specs=[whole(pltpu.SMEM)] + [whole()] * 4,
        out_specs=whole(),
        name="down",
    )(at_core, hidden, swap(hidden, "c"), w_down, swap(w_down, "c"))
    parts = parts.reshape(n_sp * n_y, capacity, feat_block)
    returned = lax.all_to_all(parts, ("sp", "y"), 0, 0, tiled=True)
    returned = returned.reshape(experts, n_y, capacity, feat_block)
    expert_out = jnp.sum(returned.astype(f32), 1).astype(bf16).reshape(experts * capacity, feat_block)
    first = (slot_index[:, :1] == slots[None, :]).astype(bf16)
    second = (slot_index[:, 1:] == slots[None, :]).astype(bf16)
    moe_sum = route_weights[:, :1] * jnp.dot(
        first, expert_out, preferred_element_type=f32
    ) + route_weights[:, 1:] * jnp.dot(second, expert_out, preferred_element_type=f32)

    own_gain = lax.dynamic_slice_in_dim(mix_gain, at_tp * feat_block, feat_block, 0)[None]
    z_gain = own_z * own_gain
    sums = jnp.stack(
        [
            jnp.sum(own_z, 1),
            jnp.sum(own_z * own_z, 1),
            jnp.sum(z_gain, 1),
            jnp.sum(z_gain * z_gain, 1),
            jnp.sum(z_gain * own_gain, 1),
            jnp.sum(z_gain * moe_sum, 1),
            jnp.sum(own_gain * moe_sum, 1),
            jnp.sum(moe_sum, 1),
            jnp.sum(moe_sum * moe_sum, 1),
            jnp.zeros_like(moe_sum[:, 0]),
        ]
    )
    sums = summed_over(sums.reshape(-1, 128), TP, n_tp).reshape(10, tok_rows)
    z_mean = sums[0] / features
    z_rstd = lax.rsqrt(sums[1] / features - z_mean * z_mean + norm_eps)
    ar = residual_alpha * z_rstd
    fin_sum = ar * (sums[2] - z_mean * jnp.sum(mix_gain)) + sums[7]
    fin_square = (
        ar * ar * (sums[3] - 2.0 * z_mean * sums[4] + z_mean * z_mean * jnp.sum(mix_gain * mix_gain))
        + 2.0 * ar * (sums[5] - z_mean * sums[6])
        + sums[8]
    )
    fin_mean = fin_sum / features
    fin_rstd = lax.rsqrt(fin_square / features - fin_mean * fin_mean + norm_eps)
    pre_norm = ar[:, None] * (own_z - z_mean[:, None]) * own_gain + moe_sum
    return ((pre_norm - fin_mean[:, None]) * fin_rstd[:, None] * final_gain).astype(bf16)


def solution(mesh):
    finer = Mesh(mesh.devices.reshape(mesh.shape["sp"], 8, 2), ("sp", "y", "c"))
    placed = (
        P("sp", TP),
        P("sp", TP),
        P("sp"),
        P(None, TP),
        P(TP),
        P(TP, None),
        P("sp", None),
        P(),
        P("sp", None),
        P("sp", None),
        P("sp", None, TP),
        P("sp", None, TP),
        P("sp", TP, None),
        P(TP),
    )
    return jax.shard_map(local, mesh=finer, in_specs=placed, out_specs=P("sp", TP), check_vma=False)
```

```python
import functools

import jax
import jax.numpy as jnp
from jax import lax
from jax.experimental import pallas as pl
from jax.experimental.pallas import tpu as pltpu
from jax.sharding import Mesh
from jax.sharding import PartitionSpec as P

TP = ("y", "c")

residual_alpha = 1.41421356
norm_eps = 1e-05
row_scale = 64.0


def from_behind(value, axis, by):
    peers = lax.axis_size(axis)
    pairs = [(i, i + by) for i in range(peers) if 0 <= i + by < peers]
    return lax.ppermute(value, axis, pairs)


def swap(value, axis):
    return lax.ppermute(value, axis, [(0, 1), (1, 0)])


def summed_over(value, axis, peers):
    copies = jnp.broadcast_to(value[None], (peers, *value.shape))
    return jnp.sum(lax.all_to_all(copies, axis, 0, 0, tiled=True), axis=0)


def conv_body(packed_ref, ids_ref, out_ref, *, lags, tok_rows):
    packed = packed_ref[...]
    ids = ids_ref[...]
    lane = lax.broadcasted_iota(jnp.int32, packed.shape, 1)
    total = jnp.zeros_like(packed)
    for lag in range(lags):
        rows = packed if lag == 0 else pltpu.roll(packed, lag, 1)
        other = ids if lag == 0 else pltpu.roll(ids, lag, 1)
        tap = packed[:, tok_rows + lag : tok_rows + lag + 1]
        total = total + jnp.where(other[:1] == ids[:1], rows, 0.0) * tap
    left = packed[:, tok_rows + lags : tok_rows + lags + 1]
    out = jnp.where(lane < tok_rows, total, 0.0).astype(jnp.bfloat16).astype(jnp.float32)
    for piece in range(3):
        rounded = left.astype(jnp.bfloat16).astype(jnp.float32)
        out = jnp.where(lane == tok_rows + piece, rounded, out)
        left = left - rounded
    out_ref[...] = out.astype(jnp.bfloat16)


def mix_body(slot_ref, filtered_ref, weight_ref, residual_ref, z_ref, out_ref):
    channels = filtered_ref.shape[0]
    tok_rows = z_ref.shape[0]
    filtered = filtered_ref[...].astype(jnp.float32)
    gain = jnp.sum(filtered[:, tok_rows : tok_rows + 3], 1, keepdims=True)
    filtered = filtered[:, :tok_rows]
    row_mean = jnp.sum(filtered, 0, keepdims=True) / channels
    row_var = jnp.sum(filtered * filtered, 0, keepdims=True) / channels - row_mean * row_mean
    normed = (filtered - row_mean) * lax.rsqrt(row_var + norm_eps) * gain
    conv_out = (normed / (1.0 + jnp.exp(-normed))).astype(jnp.bfloat16)
    mix = lax.dot_general(
        conv_out, weight_ref[...], (((0,), (0,)), ((), ())), preferred_element_type=jnp.float32
    )
    z = residual_alpha * residual_ref[...].astype(jnp.float32) + mix
    z_ref[...] = z
    experts, capacity, block = out_ref.shape
    slot = lax.broadcasted_iota(jnp.int32, (experts * capacity, tok_rows), 0)
    table = (slot == slot_ref[:1]) | (slot == slot_ref[1:2])
    outgoing = jnp.dot(
        jnp.where(table, 1.0, 0.0).astype(jnp.bfloat16),
        z.astype(jnp.bfloat16),
        preferred_element_type=jnp.float32,
    )
    out_ref[...] = outgoing.astype(jnp.bfloat16).reshape(experts, capacity, block)


def down_body(at_ref, mine_ref, else_ref, down_mine_ref, down_else_ref, out_ref):
    n_sp, peers, capacity, block = out_ref.shape
    hidden = jnp.concatenate([mine_ref[...], else_ref[...]], 0)
    for peer in range(0, peers, 2):
        columns = []
        for step in range(2):
            at = pl.multiple_of((2 * (peer + step) + at_ref[0]) * block, block)
            columns.append(
                jnp.concatenate([down_mine_ref[:, pl.ds(at, block)], down_else_ref[:, pl.ds(at, block)]], 0)
            )
        part = lax.dot_general(
            hidden,
            jnp.concatenate(columns, 1),
            (((0,), (0,)), ((), ())),
            preferred_element_type=jnp.float32,
        ).astype(jnp.bfloat16)
        out_ref[:, peer] = part[:, :block].reshape(n_sp, capacity, block)
        out_ref[:, peer + 1] = part[:, block:].reshape(n_sp, capacity, block)


def whole(memory=None):
    return pl.BlockSpec(memory_space=memory or pltpu.VMEM)


def local(
    glu_value,
    glu_gate,
    doc_ids,
    conv_kernel,
    conv_gain,
    out_weight,
    residual,
    mix_gain,
    routes,
    route_weights,
    expert_gate,
    expert_up,
    expert_down,
    final_gain,
):
    f32, bf16 = jnp.float32, jnp.bfloat16
    n_sp, n_y, n_c = lax.axis_size("sp"), lax.axis_size("y"), lax.axis_size("c")
    n_tp = n_y * n_c
    at_core = lax.axis_index("c").astype(jnp.int32).reshape(1)
    at_tp = lax.axis_index(TP)
    tok_rows, own_ch = glu_value.shape
    lags = conv_kernel.shape[0]
    rim_len = lags - 1
    features = residual.shape[1]
    feat_block = features // n_tp

    value, gate = glu_value.T.astype(f32), glu_gate.T.astype(f32)
    gated = (value * jax.nn.sigmoid(gate)).astype(bf16)
    ids = doc_ids.astype(f32)[None]
    rim = jnp.concatenate([gated[:, tok_rows - rim_len :], ids[:, tok_rows - rim_len :].astype(bf16)], 0)
    rim = from_behind(rim, "sp", 1).astype(f32)
    lanes = 256
    blank = lanes - tok_rows - lags - 1 - rim_len
    packed = jnp.concatenate(
        [
            gated.astype(f32),
            conv_kernel.T.astype(f32),
            conv_gain[:, None],
            jnp.zeros((own_ch, blank), f32),
            rim[:own_ch],
        ],
        1,
    )
    packed_ids = jnp.concatenate(
        [ids, jnp.zeros((1, lanes - tok_rows - rim_len), f32), rim[own_ch:]], 1
    )
    packed_ids = jnp.broadcast_to(packed_ids, (8, lanes))
    filtered = pl.pallas_call(
        functools.partial(conv_body, lags=lags, tok_rows=tok_rows),
        out_shape=jax.ShapeDtypeStruct((own_ch, lanes), bf16),
        in_specs=[whole()] * 2,
        out_specs=whole(),
        name="conv",
    )(packed, packed_ids)
    filtered = lax.all_gather(filtered, TP, axis=0, tiled=True)
    weight_parts = out_weight.reshape(own_ch, n_tp, feat_block).transpose(1, 0, 2)
    weight_own = lax.all_to_all(weight_parts, TP, 0, 0, tiled=True).reshape(-1, feat_block)
    own_residual = lax.dynamic_slice_in_dim(residual, at_tp * feat_block, feat_block, 1)

    experts = expert_gate.shape[0] * n_sp
    capacity = 4 * tok_rows // experts
    chosen = routes.reshape(-1)
    member = (chosen[:, None] == jnp.arange(experts, dtype=jnp.int32)[None, :]).astype(jnp.int32)
    earlier = jnp.cumsum(member, 0) - member
    slot_index = (chosen * capacity + jnp.sum(earlier * member, 1)).reshape(tok_rows, 2)
    slots = jnp.arange(experts * capacity, dtype=jnp.int32)
    slot_rows = jnp.concatenate([slot_index.T, jnp.zeros((6, tok_rows), jnp.int32)], 0)

    own_z, outgoing = pl.pallas_call(
        mix_body,
        out_shape=(
            jax.ShapeDtypeStruct((tok_rows, feat_block), f32),
            jax.ShapeDtypeStruct((experts, capacity, feat_block), bf16),
        ),
        in_specs=[whole()] * 4,
        out_specs=(whole(), whole()),
        name="mix",
    )(slot_rows, filtered, weight_own, own_residual)
    arrived = lax.all_to_all(outgoing, "sp", 0, 0, tiled=True)
    rows = n_sp * capacity
    arrived = (arrived.reshape(rows, feat_block).T.astype(f32) * row_scale).astype(jnp.float16)
    gathered = lax.all_gather(arrived, TP, axis=0, tiled=True)

    wide = gathered.astype(f32)
    in_mean = jnp.sum(wide, 0) * (1.0 / (row_scale * features))
    in_square = jnp.sum(wide * wide, 0) * (1.0 / (row_scale * row_scale * features))
    in_rstd = lax.rsqrt(in_square - in_mean * in_mean + norm_eps)
    in_rows = (
        (wide * (1.0 / row_scale) - in_mean[None]) * in_rstd[None] * mix_gain[:, None]
    ).astype(bf16)
    gate_proj = jnp.einsum("kf,kr->fr", expert_gate[0], in_rows, preferred_element_type=f32)
    up_proj = jnp.einsum("kf,kr->fr", expert_up[0], in_rows, preferred_element_type=f32)
    hidden = (jax.nn.silu(gate_proj) * up_proj).astype(bf16)

    w_down = expert_down[0]
    parts = pl.pallas_call(
        down_body,
        out_shape=jax.ShapeDtypeStruct((n_sp, n_y, capacity, feat_block), bf16),
        in_specs=[whole(pltpu.SMEM)] + [whole()] * 4,
        out_specs=whole(),
        name="down",
    )(at_core, hidden, swap(hidden, "c"), w_down, swap(w_down, "c"))
    parts = parts.reshape(n_sp * n_y, capacity, feat_block)
    returned = lax.all_to_all(parts, ("sp", "y"), 0, 0, tiled=True)
    returned = returned.reshape(experts, n_y, capacity, feat_block)
    expert_out = jnp.sum(returned.astype(f32), 1).astype(bf16).reshape(experts * capacity, feat_block)
    first = (slot_index[:, :1] == slots[None, :]).astype(bf16)
    second = (slot_index[:, 1:] == slots[None, :]).astype(bf16)
    moe_sum = route_weights[:, :1] * jnp.dot(
        first, expert_out, preferred_element_type=f32
    ) + route_weights[:, 1:] * jnp.dot(second, expert_out, preferred_element_type=f32)

    own_gain = lax.dynamic_slice_in_dim(mix_gain, at_tp * feat_block, feat_block, 0)[None]
    z_gain = own_z * own_gain
    sums = jnp.stack(
        [
            jnp.sum(own_z, 1),
            jnp.sum(own_z * own_z, 1),
            jnp.sum(z_gain, 1),
            jnp.sum(z_gain * z_gain, 1),
            jnp.sum(z_gain * own_gain, 1),
            jnp.sum(z_gain * moe_sum, 1),
            jnp.sum(own_gain * moe_sum, 1),
            jnp.sum(moe_sum, 1),
            jnp.sum(moe_sum * moe_sum, 1),
            jnp.zeros_like(moe_sum[:, 0]),
        ]
    )
    sums = summed_over(sums.reshape(-1, 128), TP, n_tp).reshape(10, tok_rows)
    z_mean = sums[0] / features
    z_rstd = lax.rsqrt(sums[1] / features - z_mean * z_mean + norm_eps)
    ar = residual_alpha * z_rstd
    fin_sum = ar * (sums[2] - z_mean * jnp.sum(mix_gain)) + sums[7]
    fin_square = (
        ar * ar * (sums[3] - 2.0 * z_mean * sums[4] + z_mean * z_mean * jnp.sum(mix_gain * mix_gain))
        + 2.0 * ar * (sums[5] - z_mean * sums[6])
        + sums[8]
    )
    fin_mean = fin_sum / features
    fin_rstd = lax.rsqrt(fin_square / features - fin_mean * fin_mean + norm_eps)
    pre_norm = ar[:, None] * (own_z - z_mean[:, None]) * own_gain + moe_sum
    return ((pre_norm - fin_mean[:, None]) * fin_rstd[:, None] * final_gain).astype(bf16)


def solution(mesh):
    finer = Mesh(mesh.devices.reshape(mesh.shape["sp"], 8, 2), ("sp", "y", "c"))
    placed = (
        P("sp", TP),
        P("sp", TP),
        P("sp"),
        P(None, TP),
        P(TP),
        P(TP, None),
        P("sp", None),
        P(),
        P("sp", None),
        P("sp", None),
        P("sp", None, TP),
        P("sp", None, TP),
        P("sp", TP, None),
        P(TP),
    )
    return jax.shard_map(local, mesh=finer, in_specs=placed, out_specs=P("sp", TP), check_vma=False)
```

```python
import functools

import jax
import jax.numpy as jnp
from jax import lax
from jax.experimental import pallas as pl
from jax.experimental.pallas import tpu as pltpu
from jax.sharding import Mesh
from jax.sharding import PartitionSpec as P

TP = ("y", "c")

residual_alpha = 1.41421356
norm_eps = 1e-05
row_scale = 64.0


def from_behind(value, axis, by):
    peers = lax.axis_size(axis)
    pairs = [(i, i + by) for i in range(peers) if 0 <= i + by < peers]
    return lax.ppermute(value, axis, pairs)


def swap(value, axis):
    return lax.ppermute(value, axis, [(0, 1), (1, 0)])


def summed_over(value, axis, peers):
    copies = jnp.broadcast_to(value[None], (peers, *value.shape))
    return jnp.sum(lax.all_to_all(copies, axis, 0, 0, tiled=True), axis=0)


def head_body(value_ref, gate_ref, ids_ref, own_ref, rim_ref):
    own_ch, tok_rows = value_ref.shape
    gate = gate_ref[...].astype(jnp.float32)
    gated = value_ref[...].astype(jnp.float32) * (1.0 / (1.0 + jnp.exp(-gate)))
    gated = gated.astype(jnp.bfloat16).astype(jnp.float32)
    ids = jnp.broadcast_to(ids_ref[...].astype(jnp.float32), (own_ref.shape[0] - own_ch, tok_rows))
    rows = jnp.concatenate([gated, ids], 0)
    rows = jnp.concatenate([rows, jnp.zeros((rows.shape[0], own_ref.shape[1] - tok_rows), jnp.float32)], 1)
    own_ref[...] = rows.astype(jnp.bfloat16)
    shifted = pltpu.roll(rows, own_ref.shape[1] - (tok_rows - 128), 1)
    rim_ref[...] = shifted[:, :128].astype(jnp.bfloat16)


def conv_body(own_ref, rim_ref, taps_ref, out_ref, *, lags, tok_rows):
    own_ch = out_ref.shape[0]
    own = own_ref[...].astype(jnp.float32)
    rim = rim_ref[...].astype(jnp.float32)
    lane = lax.broadcasted_iota(jnp.int32, rim.shape, 1)
    behind = jnp.where(lane < tok_rows - 128, own[:, 128:], rim)
    packed = jnp.concatenate([own[:, :128], behind], 1)
    rows, ids = packed[:own_ch], packed[own_ch : own_ch + 8]
    taps = taps_ref[...]
    total = jnp.zeros_like(rows)
    for lag in range(lags):
        moved = rows if lag == 0 else pltpu.roll(rows, lag, 1)
        other = ids if lag == 0 else pltpu.roll(ids, lag, 1)
        total = total + jnp.where(other[:1] == ids[:1], moved, 0.0) * taps[:, lag : lag + 1]
    left = taps[:, lags : lags + 1]
    lane = lax.broadcasted_iota(jnp.int32, rows.shape, 1)
    out = jnp.where(lane < tok_rows, total, 0.0).astype(jnp.bfloat16).astype(jnp.float32)
    for piece in range(3):
        rounded = left.astype(jnp.bfloat16).astype(jnp.float32)
        out = jnp.where(lane == tok_rows + piece, rounded, out)
        left = left - rounded
    out_ref[...] = out.astype(jnp.bfloat16)


def mix_body(at_ref, routes_ref, filtered_ref, weight_ref, residual_ref, z_ref, out_ref, slot_ref):
    channels = filtered_ref.shape[0]
    tok_rows = z_ref.shape[0]
    experts, capacity, block = out_ref.shape
    expert = lax.broadcasted_iota(jnp.int32, (experts, tok_rows), 0)
    named = [expert == routes_ref[pick : pick + 1] for pick in range(2)]
    earlier = lax.broadcasted_iota(jnp.int32, (tok_rows, tok_rows), 0) < lax.broadcasted_iota(
        jnp.int32, (tok_rows, tok_rows), 1
    )
    rank = jnp.dot(
        jnp.where(named[0] | named[1], 1.0, 0.0).astype(jnp.bfloat16),
        jnp.where(earlier, 1.0, 0.0).astype(jnp.bfloat16),
        preferred_element_type=jnp.float32,
    )
    place = expert.astype(jnp.float32) * capacity + rank
    slots = [
        jnp.sum(jnp.where(who, place, 0.0), 0, keepdims=True).astype(jnp.int32) for who in named
    ]
    slot_ref[:1] = slots[0]
    slot_ref[1:2] = slots[1]

    filtered = filtered_ref[...].astype(jnp.float32)
    gain = jnp.sum(filtered[:, tok_rows : tok_rows + 3], 1, keepdims=True)
    filtered = filtered[:, :tok_rows]
    row_mean = jnp.sum(filtered, 0, keepdims=True) / channels
    row_var = jnp.sum(filtered * filtered, 0, keepdims=True) / channels - row_mean * row_mean
    normed = (filtered - row_mean) * lax.rsqrt(row_var + norm_eps) * gain
    conv_out = (normed / (1.0 + jnp.exp(-normed))).astype(jnp.bfloat16)
    mix = lax.dot_general(
        conv_out, weight_ref[...], (((0,), (0,)), ((), ())), preferred_element_type=jnp.float32
    )
    z = residual_alpha * residual_ref[...].astype(jnp.float32) + mix
    z_ref[...] = z
    slot = lax.broadcasted_iota(jnp.int32, (experts * capacity, tok_rows), 0)
    table = (slot == slots[0]) | (slot == slots[1])
    outgoing = jnp.dot(
        jnp.where(table, 1.0, 0.0).astype(jnp.bfloat16),
        z.astype(jnp.bfloat16),
        preferred_element_type=jnp.float32,
    )
    out_ref[...] = outgoing.astype(jnp.bfloat16).reshape(experts, capacity, block)


def down_body(at_ref, mine_ref, else_ref, mine_0, mine_1, else_0, else_1, out_ref, hidden_ref):
    block = out_ref.shape[2]

    @pl.when(pl.program_id(0) == 0)
    def _():
        hidden_ref[...] = jnp.concatenate([mine_ref[...], else_ref[...]], 0).T

    down = jnp.concatenate(
        [
            jnp.concatenate([mine_0[...], else_0[...]], 0),
            jnp.concatenate([mine_1[...], else_1[...]], 0),
        ],
        1,
    )
    part = jnp.dot(hidden_ref[...], down, preferred_element_type=jnp.float32).astype(jnp.bfloat16)
    out_ref[0] = part[:, :block]
    out_ref[1] = part[:, block:]


def whole(memory=None):
    return pl.BlockSpec(memory_space=memory or pltpu.VMEM)


def full(*shape):
    return pl.BlockSpec(shape, lambda *_: (0,) * len(shape))


def local(
    glu_value,
    glu_gate,
    doc_ids,
    conv_kernel,
    conv_gain,
    out_weight,
    residual,
    mix_gain,
    routes,
    route_weights,
    expert_gate,
    expert_up,
    expert_down,
    final_gain,
):
    f32, bf16 = jnp.float32, jnp.bfloat16
    n_sp, n_y, n_c = lax.axis_size("sp"), lax.axis_size("y"), lax.axis_size("c")
    n_tp = n_y * n_c
    at_core = lax.axis_index("c").astype(jnp.int32).reshape(1)
    at_tp = lax.axis_index(TP)
    tok_rows, own_ch = glu_value.shape
    features = residual.shape[1]
    feat_block = features // n_tp

    lanes, more = 256, 16
    own_rows, rim = pl.pallas_call(
        head_body,
        out_shape=(
            jax.ShapeDtypeStruct((own_ch + more, lanes), bf16),
            jax.ShapeDtypeStruct((own_ch + more, 128), bf16),
        ),
        in_specs=[whole()] * 3,
        out_specs=(whole(), whole()),
        name="head",
    )(glu_value.T, glu_gate.T, doc_ids[None])
    rim, own_rows, out_weight = lax.optimization_barrier((rim, own_rows, out_weight))
    rim = from_behind(rim, "sp", 1)
    taps = jnp.concatenate([conv_kernel.astype(f32), conv_gain[None]], 0).T
    filtered = pl.pallas_call(
        functools.partial(conv_body, lags=conv_kernel.shape[0], tok_rows=tok_rows),
        out_shape=jax.ShapeDtypeStruct((own_ch, lanes), bf16),
        in_specs=[whole()] * 3,
        out_specs=whole(),
        name="conv",
    )(own_rows, rim, taps)
    filtered = lax.all_gather(filtered, TP, axis=0, tiled=True)
    weight_parts = out_weight.reshape(own_ch, n_tp, feat_block).transpose(1, 0, 2)
    weight_own = lax.all_to_all(weight_parts, TP, 0, 0, tiled=True).reshape(-1, feat_block)
    experts = expert_gate.shape[0] * n_sp
    capacity = 4 * tok_rows // experts
    own_z, outgoing, slot_rows = pl.pallas_call(
        mix_body,
        out_shape=(
            jax.ShapeDtypeStruct((tok_rows, feat_block), f32),
            jax.ShapeDtypeStruct((experts, capacity, feat_block), bf16),
            jax.ShapeDtypeStruct((2, tok_rows), jnp.int32),
        ),
        grid_spec=pltpu.PrefetchScalarGridSpec(
            num_scalar_prefetch=1,
            grid=(1,),
            in_specs=[
                full(2, tok_rows),
                full(own_ch * n_tp, lanes),
                full(own_ch * n_tp, feat_block),
                pl.BlockSpec((tok_rows, feat_block), lambda i, at: (0, at[0])),
            ],
            out_specs=(
                full(tok_rows, feat_block),
                full(experts, capacity, feat_block),
                full(2, tok_rows),
            ),
        ),
        name="mix",
    )(at_tp.astype(jnp.int32).reshape(1), routes.T, filtered, weight_own, residual)
    arrived = lax.all_to_all(outgoing, "sp", 0, 0, tiled=True)
    rows = n_sp * capacity
    arrived = (arrived.reshape(rows, feat_block).T.astype(f32) * row_scale).astype(jnp.float16)
    gathered = lax.all_gather(arrived, TP, axis=0, tiled=True)

    wide = gathered.astype(f32)
    in_mean = jnp.sum(wide, 0) * (1.0 / (row_scale * features))
    in_square = jnp.sum(wide * wide, 0) * (1.0 / (row_scale * row_scale * features))
    in_rstd = lax.rsqrt(in_square - in_mean * in_mean + norm_eps)
    in_rows = (
        (wide * (1.0 / row_scale) - in_mean[None]) * in_rstd[None] * mix_gain[:, None]
    ).astype(bf16)
    gate_proj = jnp.einsum("kf,kr->fr", expert_gate[0], in_rows, preferred_element_type=f32)
    up_proj = jnp.einsum("kf,kr->fr", expert_up[0], in_rows, preferred_element_type=f32)
    hidden = (jax.nn.silu(gate_proj) * up_proj).astype(bf16)

    w_down = expert_down[0]
    units = w_down.shape[0]
    picks = [
        pl.BlockSpec((units, feat_block), lambda i, at, step=step: (0, 2 * (2 * i + step) + at[0]))
        for step in range(2)
    ]
    parts = pl.pallas_call(
        down_body,
        out_shape=jax.ShapeDtypeStruct((n_y, rows, feat_block), bf16),
        grid_spec=pltpu.PrefetchScalarGridSpec(
            num_scalar_prefetch=1,
            grid=(n_y // 2,),
            in_specs=[full(units, rows), full(units, rows), *picks, *picks],
            out_specs=pl.BlockSpec((2, rows, feat_block), lambda i, at: (i, 0, 0)),
            scratch_shapes=[pltpu.VMEM((rows, n_c * units), bf16)],
        ),
        name="down",
    )(at_core, hidden, swap(hidden, "c"), w_down, w_down, *([swap(w_down, "c")] * 2))
    parts = lax.all_to_all(parts, "y", 0, 0, tiled=True)
    summed = jnp.sum(parts.astype(f32), 0).astype(bf16).reshape(n_sp, capacity, feat_block)
    expert_out = lax.all_to_all(summed, "sp", 0, 0, tiled=True).reshape(rows, feat_block)
    slots = jnp.arange(experts * capacity, dtype=jnp.int32)
    first = (slot_rows[0][:, None] == slots[None, :]).astype(bf16)
    second = (slot_rows[1][:, None] == slots[None, :]).astype(bf16)
    moe_sum = route_weights[:, :1] * jnp.dot(
        first, expert_out, preferred_element_type=f32
    ) + route_weights[:, 1:] * jnp.dot(second, expert_out, preferred_element_type=f32)

    own_gain = lax.dynamic_slice_in_dim(mix_gain, at_tp * feat_block, feat_block, 0)[None]
    z_gain = own_z * own_gain
    sums = jnp.stack(
        [
            jnp.sum(own_z, 1),
            jnp.sum(own_z * own_z, 1),
            jnp.sum(z_gain, 1),
            jnp.sum(z_gain * z_gain, 1),
            jnp.sum(z_gain * own_gain, 1),
            jnp.sum(z_gain * moe_sum, 1),
            jnp.sum(own_gain * moe_sum, 1),
            jnp.sum(moe_sum, 1),
            jnp.sum(moe_sum * moe_sum, 1),
            jnp.zeros_like(moe_sum[:, 0]),
        ]
    )
    sums = summed_over(sums.reshape(-1, 128), TP, n_tp).reshape(10, tok_rows)
    z_mean = sums[0] / features
    z_rstd = lax.rsqrt(sums[1] / features - z_mean * z_mean + norm_eps)
    ar = residual_alpha * z_rstd
    fin_sum = ar * (sums[2] - z_mean * jnp.sum(mix_gain)) + sums[7]
    fin_square = (
        ar * ar * (sums[3] - 2.0 * z_mean * sums[4] + z_mean * z_mean * jnp.sum(mix_gain * mix_gain))
        + 2.0 * ar * (sums[5] - z_mean * sums[6])
        + sums[8]
    )
    fin_mean = fin_sum / features
    fin_rstd = lax.rsqrt(fin_square / features - fin_mean * fin_mean + norm_eps)
    pre_norm = ar[:, None] * (own_z - z_mean[:, None]) * own_gain + moe_sum
    return ((pre_norm - fin_mean[:, None]) * fin_rstd[:, None] * final_gain).astype(bf16)


def solution(mesh):
    finer = Mesh(mesh.devices.reshape(mesh.shape["sp"], 8, 2), ("sp", "y", "c"))
    placed = (
        P("sp", TP),
        P("sp", TP),
        P("sp"),
        P(None, TP),
        P(TP),
        P(TP, None),
        P("sp", None),
        P(),
        P("sp", None),
        P("sp", None),
        P("sp", None, TP),
        P("sp", None, TP),
        P("sp", TP, None),
        P(TP),
    )
    return jax.shard_map(local, mesh=finer, in_specs=placed, out_specs=P("sp", TP), check_vma=False)
```

```python
import functools

import jax
import jax.numpy as jnp
from jax import lax
from jax.experimental import pallas as pl
from jax.experimental.pallas import tpu as pltpu
from jax.sharding import Mesh
from jax.sharding import PartitionSpec as P


TP = ("y", "c")

residual_alpha = 1.41421356
norm_eps = 1e-05
row_scale = 64.0


def from_behind(value, axis, by):
    peers = lax.axis_size(axis)
    pairs = [(i, i + by) for i in range(peers) if 0 <= i + by < peers]
    return lax.ppermute(value, axis, pairs)


def swap(value, axis):
    return lax.ppermute(value, axis, [(0, 1), (1, 0)])


def summed_over(value, axis, peers):
    copies = jnp.broadcast_to(value[None], (peers, *value.shape))
    return jnp.sum(lax.all_to_all(copies, axis, 0, 0, tiled=True), axis=0)


def head_body(value_ref, gate_ref, ids_ref, own_ref, rim_ref):
    own_ch, tok_rows = value_ref.shape
    gate = gate_ref[...].astype(jnp.float32)
    gated = value_ref[...].astype(jnp.float32) * (1.0 / (1.0 + jnp.exp(-gate)))
    gated = gated.astype(jnp.bfloat16).astype(jnp.float32)
    ids = jnp.broadcast_to(ids_ref[...].astype(jnp.float32), (own_ref.shape[0] - own_ch, tok_rows))
    rows = jnp.concatenate([gated, ids], 0)
    rows = jnp.concatenate([rows, jnp.zeros((rows.shape[0], own_ref.shape[1] - tok_rows), jnp.float32)], 1)
    own_ref[...] = rows.astype(jnp.bfloat16)
    shifted = pltpu.roll(rows, own_ref.shape[1] - (tok_rows - 128), 1)
    rim_ref[...] = shifted[:, :128].astype(jnp.bfloat16)


def conv_body(own_ref, rim_ref, kernel_ref, gain_ref, out_ref, *, lags, tok_rows):
    own_ch = out_ref.shape[0]
    own = own_ref[...].astype(jnp.float32)
    rim = rim_ref[...].astype(jnp.float32)
    lane = lax.broadcasted_iota(jnp.int32, rim.shape, 1)
    behind = jnp.where(lane < tok_rows - 128, own[:, 128:], rim)
    packed = jnp.concatenate([own[:, :128], behind], 1)
    rows, ids = packed[:own_ch], packed[own_ch : own_ch + 8]
    taps = jnp.concatenate([kernel_ref[...].astype(jnp.float32), gain_ref[...]], 0).T
    total = jnp.zeros_like(rows)
    for lag in range(lags):
        moved = rows if lag == 0 else pltpu.roll(rows, lag, 1)
        other = ids if lag == 0 else pltpu.roll(ids, lag, 1)
        total = total + jnp.where(other[:1] == ids[:1], moved, 0.0) * taps[:, lag : lag + 1]
    left = taps[:, lags : lags + 1]
    lane = lax.broadcasted_iota(jnp.int32, rows.shape, 1)
    out = jnp.where(lane < tok_rows, total, 0.0).astype(jnp.bfloat16).astype(jnp.float32)
    for piece in range(3):
        rounded = left.astype(jnp.bfloat16).astype(jnp.float32)
        out = jnp.where(lane == tok_rows + piece, rounded, out)
        left = left - rounded
    out_ref[...] = out.astype(jnp.bfloat16)


def mix_body(at_ref, routes_ref, filtered_ref, weight_ref, residual_ref, z_ref, out_ref, slot_ref):
    channels = filtered_ref.shape[0]
    tok_rows = z_ref.shape[0]
    experts, capacity, block = out_ref.shape
    expert = lax.broadcasted_iota(jnp.int32, (experts, tok_rows), 0)
    named = [expert == routes_ref[pick : pick + 1] for pick in range(2)]
    earlier = lax.broadcasted_iota(jnp.int32, (tok_rows, tok_rows), 0) < lax.broadcasted_iota(
        jnp.int32, (tok_rows, tok_rows), 1
    )
    rank = jnp.dot(
        jnp.where(named[0] | named[1], 1.0, 0.0).astype(jnp.bfloat16),
        jnp.where(earlier, 1.0, 0.0).astype(jnp.bfloat16),
        preferred_element_type=jnp.float32,
    )
    place = expert.astype(jnp.float32) * capacity + rank
    slots = [
        jnp.sum(jnp.where(who, place, 0.0), 0, keepdims=True).astype(jnp.int32) for who in named
    ]
    slot_ref[:1] = slots[0]
    slot_ref[1:2] = slots[1]

    filtered = filtered_ref[...].astype(jnp.float32)
    gain = jnp.sum(filtered[:, tok_rows : tok_rows + 3], 1, keepdims=True)
    filtered = filtered[:, :tok_rows]
    row_mean = jnp.sum(filtered, 0, keepdims=True) / channels
    row_var = jnp.sum(filtered * filtered, 0, keepdims=True) / channels - row_mean * row_mean
    normed = (filtered - row_mean) * lax.rsqrt(row_var + norm_eps) * gain
    conv_out = (normed / (1.0 + jnp.exp(-normed))).astype(jnp.bfloat16)
    mix = lax.dot_general(
        conv_out, weight_ref[...], (((0,), (0,)), ((), ())), preferred_element_type=jnp.float32
    )
    z = residual_alpha * residual_ref[...].astype(jnp.float32) + mix
    z_ref[...] = z
    slot = lax.broadcasted_iota(jnp.int32, (experts * capacity, tok_rows), 0)
    table = (slot == slots[0]) | (slot == slots[1])
    outgoing = jnp.dot(
        jnp.where(table, 1.0, 0.0).astype(jnp.bfloat16),
        z.astype(jnp.bfloat16),
        preferred_element_type=jnp.float32,
    )
    out_ref[...] = outgoing.astype(jnp.bfloat16).reshape(experts, capacity, block)


def down_body(at_ref, mine_ref, else_ref, mine_0, mine_1, else_0, else_1, out_ref):
    units, block = mine_0.shape
    n_sp, _, capacity, _ = out_ref.shape
    part = jnp.dot(
        mine_ref[:, :units],
        jnp.concatenate([mine_0[...], mine_1[...]], 1),
        preferred_element_type=jnp.float32,
    ) + jnp.dot(
        else_ref[:, :units],
        jnp.concatenate([else_0[...], else_1[...]], 1),
        preferred_element_type=jnp.float32,
    )
    part = part.astype(jnp.bfloat16)
    out_ref[:, 0] = part[:, :block].reshape(n_sp, capacity, block)
    out_ref[:, 1] = part[:, block:].reshape(n_sp, capacity, block)


def whole(memory=None):
    return pl.BlockSpec(memory_space=memory or pltpu.VMEM)


def full(*shape):
    return pl.BlockSpec(shape, lambda *_: (0,) * len(shape))


def local(
    glu_value,
    glu_gate,
    doc_ids,
    conv_kernel,
    conv_gain,
    out_weight,
    residual,
    mix_gain,
    routes,
    route_weights,
    expert_gate,
    expert_up,
    expert_down,
    final_gain,
):
    f32, bf16 = jnp.float32, jnp.bfloat16
    n_sp, n_y, n_c = lax.axis_size("sp"), lax.axis_size("y"), lax.axis_size("c")
    n_tp = n_y * n_c
    at_core = lax.axis_index("c").astype(jnp.int32).reshape(1)
    at_tp = lax.axis_index(TP)
    tok_rows, own_ch = glu_value.shape
    features = residual.shape[1]
    feat_block = features // n_tp

    lanes, more = 256, 16
    own_rows, rim = pl.pallas_call(
        head_body,
        out_shape=(
            jax.ShapeDtypeStruct((own_ch + more, lanes), bf16),
            jax.ShapeDtypeStruct((own_ch + more, 128), bf16),
        ),
        in_specs=[whole()] * 3,
        out_specs=(whole(), whole()),
        name="head",
    )(glu_value.T, glu_gate.T, doc_ids[None])
    rim, own_rows, out_weight = lax.optimization_barrier((rim, own_rows, out_weight))
    rim = from_behind(rim, "sp", 1)
    filtered = pl.pallas_call(
        functools.partial(conv_body, lags=conv_kernel.shape[0], tok_rows=tok_rows),
        out_shape=jax.ShapeDtypeStruct((own_ch, lanes), bf16),
        in_specs=[whole()] * 4,
        out_specs=whole(),
        name="conv",
    )(own_rows, rim, conv_kernel, conv_gain[None])
    filtered = lax.all_gather(filtered, TP, axis=0, tiled=True)
    weight_parts = out_weight.reshape(own_ch, n_tp, feat_block).transpose(1, 0, 2)
    weight_own = lax.all_to_all(weight_parts, TP, 0, 0, tiled=True)
    weight_own = weight_own.reshape(-1, feat_block)
    experts = expert_gate.shape[0] * n_sp
    capacity = 4 * tok_rows // experts
    own_z, outgoing, slot_rows = pl.pallas_call(
        mix_body,
        out_shape=(
            jax.ShapeDtypeStruct((tok_rows, feat_block), f32),
            jax.ShapeDtypeStruct((experts, capacity, feat_block), bf16),
            jax.ShapeDtypeStruct((2, tok_rows), jnp.int32),
        ),
        grid_spec=pltpu.PrefetchScalarGridSpec(
            num_scalar_prefetch=1,
            grid=(1,),
            in_specs=[
                full(2, tok_rows),
                full(own_ch * n_tp, lanes),
                full(own_ch * n_tp, feat_block),
                pl.BlockSpec((tok_rows, feat_block), lambda i, at: (0, at[0])),
            ],
            out_specs=(
                full(tok_rows, feat_block),
                full(experts, capacity, feat_block),
                full(2, tok_rows),
            ),
        ),
        name="mix",
    )(at_tp.astype(jnp.int32).reshape(1), routes.T, filtered, weight_own, residual)
    arrived = lax.all_to_all(outgoing, "sp", 0, 0, tiled=True)
    rows = n_sp * capacity
    arrived = (arrived.reshape(rows, feat_block).T.astype(f32) * row_scale).astype(jnp.float16)
    gathered = lax.all_gather(arrived, TP, axis=0, tiled=True)

    wide = gathered.astype(f32)
    in_mean = jnp.sum(wide, 0) * (1.0 / (row_scale * features))
    in_square = jnp.sum(wide * wide, 0) * (1.0 / (row_scale * row_scale * features))
    in_rstd = lax.rsqrt(in_square - in_mean * in_mean + norm_eps)
    in_rows = (
        (wide * (1.0 / row_scale) - in_mean[None]) * in_rstd[None] * mix_gain[:, None]
    ).astype(bf16)
    gate_proj = jnp.einsum("kr,kf->rf", in_rows, expert_gate[0], preferred_element_type=f32)
    up_proj = jnp.einsum("kr,kf->rf", in_rows, expert_up[0], preferred_element_type=f32)
    hidden = (jax.nn.silu(gate_proj) * up_proj).astype(bf16)
    wide_units = -(-hidden.shape[1] // 128) * 128
    hidden = jnp.pad(hidden, ((0, 0), (0, wide_units - hidden.shape[1])))

    w_down = expert_down[0]
    units = w_down.shape[0]
    picks = [
        pl.BlockSpec((units, feat_block), lambda i, at, step=step: (0, 2 * (2 * i + step) + at[0]))
        for step in range(2)
    ]
    parts = pl.pallas_call(
        down_body,
        out_shape=jax.ShapeDtypeStruct((n_sp, n_y, capacity, feat_block), bf16),
        grid_spec=pltpu.PrefetchScalarGridSpec(
            num_scalar_prefetch=1,
            grid=(n_y // 2,),
            in_specs=[full(rows, wide_units), full(rows, wide_units), *picks, *picks],
            out_specs=pl.BlockSpec((n_sp, 2, capacity, feat_block), lambda i, at: (0, i, 0, 0)),
        ),
        name="down",
    )(at_core, hidden, swap(hidden, "c"), w_down, w_down, *([swap(w_down, "c")] * 2))
    parts = parts.reshape(n_sp * n_y, capacity, feat_block)
    returned = lax.all_to_all(parts, ("sp", "y"), 0, 0, tiled=True)
    returned = returned.reshape(experts, n_y, capacity, feat_block)
    expert_out = jnp.sum(returned.astype(f32), 1).astype(bf16).reshape(rows, feat_block)
    slots = jnp.arange(experts * capacity, dtype=jnp.int32)
    first = (slot_rows[0][:, None] == slots[None, :]).astype(bf16)
    second = (slot_rows[1][:, None] == slots[None, :]).astype(bf16)
    moe_sum = route_weights[:, :1] * jnp.dot(
        first, expert_out, preferred_element_type=f32
    ) + route_weights[:, 1:] * jnp.dot(second, expert_out, preferred_element_type=f32)

    own_gain = lax.dynamic_slice_in_dim(mix_gain, at_tp * feat_block, feat_block, 0)[None]
    z_gain = own_z * own_gain
    sums = jnp.stack(
        [
            jnp.sum(own_z, 1),
            jnp.sum(own_z * own_z, 1),
            jnp.sum(z_gain, 1),
            jnp.sum(z_gain * z_gain, 1),
            jnp.sum(z_gain * own_gain, 1),
            jnp.sum(z_gain * moe_sum, 1),
            jnp.sum(own_gain * moe_sum, 1),
            jnp.sum(moe_sum, 1),
            jnp.sum(moe_sum * moe_sum, 1),
            jnp.zeros_like(moe_sum[:, 0]),
        ]
    )
    sums = summed_over(sums.reshape(-1, 128), TP, n_tp).reshape(10, tok_rows)
    z_mean = sums[0] / features
    z_rstd = lax.rsqrt(sums[1] / features - z_mean * z_mean + norm_eps)
    ar = residual_alpha * z_rstd
    fin_sum = ar * (sums[2] - z_mean * jnp.sum(mix_gain)) + sums[7]
    fin_square = (
        ar * ar * (sums[3] - 2.0 * z_mean * sums[4] + z_mean * z_mean * jnp.sum(mix_gain * mix_gain))
        + 2.0 * ar * (sums[5] - z_mean * sums[6])
        + sums[8]
    )
    fin_mean = fin_sum / features
    fin_rstd = lax.rsqrt(fin_square / features - fin_mean * fin_mean + norm_eps)
    pre_norm = ar[:, None] * (own_z - z_mean[:, None]) * own_gain + moe_sum
    return ((pre_norm - fin_mean[:, None]) * fin_rstd[:, None] * final_gain).astype(bf16)


def solution(mesh):
    finer = Mesh(mesh.devices.reshape(mesh.shape["sp"], 8, 2), ("sp", "y", "c"))
    placed = (
        P("sp", TP),
        P("sp", TP),
        P("sp"),
        P(None, TP),
        P(TP),
        P(TP, None),
        P("sp", None),
        P(),
        P("sp", None),
        P("sp", None),
        P("sp", None, TP),
        P("sp", None, TP),
        P("sp", TP, None),
        P(TP),
    )
    return jax.shard_map(
        local, mesh=finer, in_specs=placed, out_specs=P("sp", TP), check_vma=False
    )
```

```python
import functools

import jax
import jax.numpy as jnp
from jax import lax
from jax.experimental import pallas as pl
from jax.experimental.pallas import tpu as pltpu
from jax.sharding import Mesh
from jax.sharding import PartitionSpec as P


Y = ("yh", "yl")
TP = ("yh", "yl", "c")

residual_alpha = 1.41421356
norm_eps = 1e-05
row_scale = 64.0


def from_behind(value, axis, by):
    peers = lax.axis_size(axis)
    pairs = [(i, i + by) for i in range(peers) if 0 <= i + by < peers]
    return lax.ppermute(value, axis, pairs)


def swap(value, axis):
    return lax.ppermute(value, axis, [(0, 1), (1, 0)])


def summed_over(value, axis, peers):
    copies = jnp.broadcast_to(value[None], (peers, *value.shape))
    return jnp.sum(lax.all_to_all(copies, axis, 0, 0, tiled=True), axis=0)


def head_body(value_ref, gate_ref, ids_ref, own_ref, rim_ref):
    own_ch, tok_rows = value_ref.shape
    gate = gate_ref[...].astype(jnp.float32)
    gated = value_ref[...].astype(jnp.float32) * (1.0 / (1.0 + jnp.exp(-gate)))
    gated = gated.astype(jnp.bfloat16).astype(jnp.float32)
    ids = jnp.broadcast_to(ids_ref[...].astype(jnp.float32), (own_ref.shape[0] - own_ch, tok_rows))
    rows = jnp.concatenate([gated, ids], 0)
    rows = jnp.concatenate([rows, jnp.zeros((rows.shape[0], own_ref.shape[1] - tok_rows), jnp.float32)], 1)
    own_ref[...] = rows.astype(jnp.bfloat16)
    shifted = pltpu.roll(rows, own_ref.shape[1] - (tok_rows - 128), 1)
    rim_ref[...] = shifted[:, :128].astype(jnp.bfloat16)


def conv_body(own_ref, rim_ref, kernel_ref, gain_ref, out_ref, *, lags, tok_rows):
    own_ch = out_ref.shape[0]
    own = own_ref[...].astype(jnp.float32)
    rim = rim_ref[...].astype(jnp.float32)
    lane = lax.broadcasted_iota(jnp.int32, rim.shape, 1)
    behind = jnp.where(lane < tok_rows - 128, own[:, 128:], rim)
    packed = jnp.concatenate([own[:, :128], behind], 1)
    rows, ids = packed[:own_ch], packed[own_ch : own_ch + 8]
    taps = jnp.concatenate([kernel_ref[...].astype(jnp.float32), gain_ref[...]], 0).T
    total = jnp.zeros_like(rows)
    for lag in range(lags):
        moved = rows if lag == 0 else pltpu.roll(rows, lag, 1)
        other = ids if lag == 0 else pltpu.roll(ids, lag, 1)
        total = total + jnp.where(other[:1] == ids[:1], moved, 0.0) * taps[:, lag : lag + 1]
    left = taps[:, lags : lags + 1]
    lane = lax.broadcasted_iota(jnp.int32, rows.shape, 1)
    out = jnp.where(lane < tok_rows, total, 0.0).astype(jnp.bfloat16).astype(jnp.float32)
    for piece in range(3):
        rounded = left.astype(jnp.bfloat16).astype(jnp.float32)
        out = jnp.where(lane == tok_rows + piece, rounded, out)
        left = left - rounded
    out_ref[...] = out.astype(jnp.bfloat16)


def mix_body(at_ref, routes_ref, filtered_ref, weight_ref, residual_ref, z_ref, out_ref, slot_ref):
    channels = filtered_ref.shape[0]
    tok_rows = z_ref.shape[0]
    experts, capacity, block = out_ref.shape
    expert = lax.broadcasted_iota(jnp.int32, (experts, tok_rows), 0)
    named = [expert == routes_ref[pick : pick + 1] for pick in range(2)]
    earlier = lax.broadcasted_iota(jnp.int32, (tok_rows, tok_rows), 0) < lax.broadcasted_iota(
        jnp.int32, (tok_rows, tok_rows), 1
    )
    rank = jnp.dot(
        jnp.where(named[0] | named[1], 1.0, 0.0).astype(jnp.bfloat16),
        jnp.where(earlier, 1.0, 0.0).astype(jnp.bfloat16),
        preferred_element_type=jnp.float32,
    )
    place = expert.astype(jnp.float32) * capacity + rank
    slots = [
        jnp.sum(jnp.where(who, place, 0.0), 0, keepdims=True).astype(jnp.int32) for who in named
    ]
    slot_ref[:1] = slots[0]
    slot_ref[1:2] = slots[1]

    filtered = filtered_ref[...].astype(jnp.float32)
    gain = jnp.sum(filtered[:, tok_rows : tok_rows + 3], 1, keepdims=True)
    filtered = filtered[:, :tok_rows]
    row_mean = jnp.sum(filtered, 0, keepdims=True) / channels
    row_var = jnp.sum(filtered * filtered, 0, keepdims=True) / channels - row_mean * row_mean
    normed = (filtered - row_mean) * lax.rsqrt(row_var + norm_eps) * gain
    conv_out = (normed / (1.0 + jnp.exp(-normed))).astype(jnp.bfloat16)
    mix = lax.dot_general(
        conv_out, weight_ref[...], (((0,), (0,)), ((), ())), preferred_element_type=jnp.float32
    )
    z = residual_alpha * residual_ref[...].astype(jnp.float32) + mix
    z_ref[...] = z
    slot = lax.broadcasted_iota(jnp.int32, (experts * capacity, tok_rows), 0)
    table = (slot == slots[0]) | (slot == slots[1])
    outgoing = jnp.dot(
        jnp.where(table, 1.0, 0.0).astype(jnp.bfloat16),
        z.astype(jnp.bfloat16),
        preferred_element_type=jnp.float32,
    )
    out_ref[...] = outgoing.astype(jnp.bfloat16).reshape(experts, capacity, block)


def down_body(at_ref, mine_ref, else_ref, *refs, picks):
    weights, outs = refs[: 2 * picks], refs[2 * picks :]
    hidden = jnp.concatenate([mine_ref[...], else_ref[...]], 0).T
    down = jnp.concatenate(
        [
            jnp.concatenate([weights[pick][...], weights[picks + pick][...]], 0)
            for pick in range(picks)
        ],
        1,
    )
    part = jnp.dot(hidden, down, preferred_element_type=jnp.float32).astype(jnp.bfloat16)
    groups, _, capacity, block = outs[0].shape
    for number, out_ref in enumerate(outs):
        rows = slice(number * groups * capacity, (number + 1) * groups * capacity)
        for pick in range(picks):
            out_ref[:, pick] = part[rows, pick * block : (pick + 1) * block].reshape(
                groups, capacity, block
            )


def whole(memory=None):
    return pl.BlockSpec(memory_space=memory or pltpu.VMEM)


def full(*shape):
    return pl.BlockSpec(shape, lambda *_: (0,) * len(shape))


def local(
    glu_value,
    glu_gate,
    doc_ids,
    conv_kernel,
    conv_gain,
    out_weight,
    residual,
    mix_gain,
    routes,
    route_weights,
    expert_gate,
    expert_up,
    expert_down,
    final_gain,
):
    f32, bf16 = jnp.float32, jnp.bfloat16
    n_sp, n_yh, n_yl, n_c = (lax.axis_size(axis) for axis in ("sp", "yh", "yl", "c"))
    n_y = n_yh * n_yl
    n_tp = n_y * n_c
    at_tp = lax.axis_index(TP)
    tok_rows, own_ch = glu_value.shape
    features = residual.shape[1]
    feat_block = features // n_tp

    lanes, more = 256, 16
    own_rows, rim = pl.pallas_call(
        head_body,
        out_shape=(
            jax.ShapeDtypeStruct((own_ch + more, lanes), bf16),
            jax.ShapeDtypeStruct((own_ch + more, 128), bf16),
        ),
        in_specs=[whole()] * 3,
        out_specs=(whole(), whole()),
        name="head",
    )(glu_value.T, glu_gate.T, doc_ids[None])
    rim, own_rows, out_weight = lax.optimization_barrier((rim, own_rows, out_weight))
    rim = from_behind(rim, "sp", 1)
    filtered = pl.pallas_call(
        functools.partial(conv_body, lags=conv_kernel.shape[0], tok_rows=tok_rows),
        out_shape=jax.ShapeDtypeStruct((own_ch, lanes), bf16),
        in_specs=[whole()] * 4,
        out_specs=whole(),
        name="conv",
    )(own_rows, rim, conv_kernel, conv_gain[None])
    filtered = lax.all_gather(filtered, TP, axis=0, tiled=True)
    weight_parts = out_weight.reshape(own_ch, n_tp, feat_block).transpose(1, 0, 2)
    weight_own = lax.all_to_all(weight_parts, TP, 0, 0, tiled=True)
    weight_own = weight_own.reshape(-1, feat_block)
    experts = expert_gate.shape[0] * n_sp
    capacity = 4 * tok_rows // experts
    own_z, outgoing, slot_rows = pl.pallas_call(
        mix_body,
        out_shape=(
            jax.ShapeDtypeStruct((tok_rows, feat_block), f32),
            jax.ShapeDtypeStruct((experts, capacity, feat_block), bf16),
            jax.ShapeDtypeStruct((2, tok_rows), jnp.int32),
        ),
        grid_spec=pltpu.PrefetchScalarGridSpec(
            num_scalar_prefetch=1,
            grid=(1,),
            in_specs=[
                full(2, tok_rows),
                full(own_ch * n_tp, lanes),
                full(own_ch * n_tp, feat_block),
                pl.BlockSpec((tok_rows, feat_block), lambda i, at: (0, at[0])),
            ],
            out_specs=(
                full(tok_rows, feat_block),
                full(experts, capacity, feat_block),
                full(2, tok_rows),
            ),
        ),
        name="mix",
    )(at_tp.astype(jnp.int32).reshape(1), routes.T, filtered, weight_own, residual)
    arrived = lax.all_to_all(outgoing, "sp", 0, 0, tiled=True)
    rows = n_sp * capacity
    arrived = (arrived.reshape(rows, feat_block).T.astype(f32) * row_scale).astype(jnp.float16)
    gathered = lax.all_gather(arrived, TP, axis=0, tiled=True)

    wide = gathered.astype(f32)
    in_mean = jnp.sum(wide, 0) * (1.0 / (row_scale * features))
    in_square = jnp.sum(wide * wide, 0) * (1.0 / (row_scale * row_scale * features))
    in_rstd = lax.rsqrt(in_square - in_mean * in_mean + norm_eps)
    in_rows = (
        (wide * (1.0 / row_scale) - in_mean[None]) * in_rstd[None] * mix_gain[:, None]
    ).astype(bf16)
    gate_proj = jnp.einsum("kf,kr->fr", expert_gate[0], in_rows, preferred_element_type=f32)
    up_proj = jnp.einsum("kf,kr->fr", expert_up[0], in_rows, preferred_element_type=f32)
    hidden = (jax.nn.silu(gate_proj) * up_proj).astype(bf16)

    w_down = expert_down[0]
    units = w_down.shape[0]
    hidden_else, down_else = swap(hidden, "c"), swap(w_down, "c")
    at_yl, at_c = lax.axis_index("yl"), lax.axis_index("c")

    def down(parity, outs):
        blocks = (jnp.arange(n_yh) * n_yl + parity) * n_c + at_c
        picks = [
            pl.BlockSpec((units, feat_block), lambda i, at, pick=pick: (0, at[pick]))
            for pick in range(n_yh)
        ]
        shape = (n_sp // outs, n_yh, capacity, feat_block)
        return pl.pallas_call(
            functools.partial(down_body, picks=n_yh),
            out_shape=[jax.ShapeDtypeStruct(shape, bf16)] * outs,
            grid_spec=pltpu.PrefetchScalarGridSpec(
                num_scalar_prefetch=1,
                grid=(1,),
                in_specs=[full(units, rows), full(units, rows), *picks, *picks],
                out_specs=[full(*shape)] * outs,
            ),
        )(blocks.astype(jnp.int32), hidden, hidden_else, *[w_down] * n_yh, *[down_else] * n_yh)

    near, far = down(1 - at_yl, 2)
    near = lax.ppermute(near, Y, [(i, i ^ 1) for i in range(n_y)])
    far = lax.ppermute(far, Y, [(i, (i - 1 if i % 2 == 0 else i + 1) % n_y) for i in range(n_y)])
    (kept,) = down(at_yl, 1)
    parts = kept.astype(f32) + jnp.concatenate([near, far], 0).astype(f32)
    parts = parts.astype(bf16).reshape(n_sp * n_yh, capacity, feat_block)
    returned = lax.all_to_all(parts, ("sp", "yh"), 0, 0, tiled=True)
    returned = returned.reshape(experts, n_yh, capacity, feat_block)
    expert_out = jnp.sum(returned.astype(f32), 1).astype(bf16).reshape(rows, feat_block)
    slots = jnp.arange(experts * capacity, dtype=jnp.int32)
    first = (slot_rows[0][:, None] == slots[None, :]).astype(bf16)
    second = (slot_rows[1][:, None] == slots[None, :]).astype(bf16)
    moe_sum = route_weights[:, :1] * jnp.dot(
        first, expert_out, preferred_element_type=f32
    ) + route_weights[:, 1:] * jnp.dot(second, expert_out, preferred_element_type=f32)

    own_gain = lax.dynamic_slice_in_dim(mix_gain, at_tp * feat_block, feat_block, 0)[None]
    z_gain = own_z * own_gain
    sums = jnp.stack(
        [
            jnp.sum(own_z, 1),
            jnp.sum(own_z * own_z, 1),
            jnp.sum(z_gain, 1),
            jnp.sum(z_gain * z_gain, 1),
            jnp.sum(z_gain * own_gain, 1),
            jnp.sum(z_gain * moe_sum, 1),
            jnp.sum(own_gain * moe_sum, 1),
            jnp.sum(moe_sum, 1),
            jnp.sum(moe_sum * moe_sum, 1),
            jnp.zeros_like(moe_sum[:, 0]),
        ]
    )
    sums = summed_over(sums.reshape(-1, 128), TP, n_tp).reshape(10, tok_rows)
    z_mean = sums[0] / features
    z_rstd = lax.rsqrt(sums[1] / features - z_mean * z_mean + norm_eps)
    ar = residual_alpha * z_rstd
    fin_sum = ar * (sums[2] - z_mean * jnp.sum(mix_gain)) + sums[7]
    fin_square = (
        ar * ar * (sums[3] - 2.0 * z_mean * sums[4] + z_mean * z_mean * jnp.sum(mix_gain * mix_gain))
        + 2.0 * ar * (sums[5] - z_mean * sums[6])
        + sums[8]
    )
    fin_mean = fin_sum / features
    fin_rstd = lax.rsqrt(fin_square / features - fin_mean * fin_mean + norm_eps)
    pre_norm = ar[:, None] * (own_z - z_mean[:, None]) * own_gain + moe_sum
    return ((pre_norm - fin_mean[:, None]) * fin_rstd[:, None] * final_gain).astype(bf16)


def solution(mesh):
    finer = Mesh(mesh.devices.reshape(mesh.shape["sp"], 4, 2, 2), ("sp", "yh", "yl", "c"))
    placed = (
        P("sp", TP),
        P("sp", TP),
        P("sp"),
        P(None, TP),
        P(TP),
        P(TP, None),
        P("sp", None),
        P(),
        P("sp", None),
        P("sp", None),
        P("sp", None, TP),
        P("sp", None, TP),
        P("sp", TP, None),
        P(TP),
    )
    return jax.shard_map(
        local, mesh=finer, in_specs=placed, out_specs=P("sp", TP), check_vma=False
    )
```

```python
import functools

import jax
import jax.numpy as jnp
from jax import lax
from jax.experimental import pallas as pl
from jax.experimental.pallas import tpu as pltpu
from jax.sharding import Mesh
from jax.sharding import PartitionSpec as P


Y = ("yh", "yl")
TP = ("yh", "yl", "c")

residual_alpha = 1.41421356
norm_eps = 1e-05
row_scale = 64.0


def from_behind(value, axis, by):
    peers = lax.axis_size(axis)
    pairs = [(i, i + by) for i in range(peers) if 0 <= i + by < peers]
    return lax.ppermute(value, axis, pairs)


def swap(value, axis):
    return lax.ppermute(value, axis, [(0, 1), (1, 0)])


def summed_over(value, axis, peers):
    copies = jnp.broadcast_to(value[None], (peers, *value.shape))
    return jnp.sum(lax.all_to_all(copies, axis, 0, 0, tiled=True), axis=0)


def head_body(value_ref, gate_ref, ids_ref, own_ref, rim_ref):
    own_ch, tok_rows = value_ref.shape
    gate = gate_ref[...].astype(jnp.float32)
    gated = value_ref[...].astype(jnp.float32) * (1.0 / (1.0 + jnp.exp(-gate)))
    gated = gated.astype(jnp.bfloat16).astype(jnp.float32)
    ids = jnp.broadcast_to(ids_ref[...].astype(jnp.float32), (own_ref.shape[0] - own_ch, tok_rows))
    rows = jnp.concatenate([gated, ids], 0)
    rows = jnp.concatenate([rows, jnp.zeros((rows.shape[0], own_ref.shape[1] - tok_rows), jnp.float32)], 1)
    own_ref[...] = rows.astype(jnp.bfloat16)
    shifted = pltpu.roll(rows, own_ref.shape[1] - (tok_rows - 128), 1)
    rim_ref[...] = shifted[:, :128].astype(jnp.bfloat16)


def conv_body(own_ref, rim_ref, kernel_ref, gain_ref, out_ref, *, lags, tok_rows):
    own_ch = out_ref.shape[0]
    own = own_ref[...].astype(jnp.float32)
    rim = rim_ref[...].astype(jnp.float32)
    lane = lax.broadcasted_iota(jnp.int32, rim.shape, 1)
    behind = jnp.where(lane < tok_rows - 128, own[:, 128:], rim)
    packed = jnp.concatenate([own[:, :128], behind], 1)
    rows, ids = packed[:own_ch], packed[own_ch : own_ch + 8]
    taps = jnp.concatenate([kernel_ref[...].astype(jnp.float32), gain_ref[...]], 0).T
    total = jnp.zeros_like(rows)
    for lag in range(lags):
        moved = rows if lag == 0 else pltpu.roll(rows, lag, 1)
        other = ids if lag == 0 else pltpu.roll(ids, lag, 1)
        total = total + jnp.where(other[:1] == ids[:1], moved, 0.0) * taps[:, lag : lag + 1]
    left = taps[:, lags : lags + 1]
    lane = lax.broadcasted_iota(jnp.int32, rows.shape, 1)
    out = jnp.where(lane < tok_rows, total, 0.0).astype(jnp.bfloat16).astype(jnp.float32)
    for piece in range(3):
        rounded = left.astype(jnp.bfloat16).astype(jnp.float32)
        out = jnp.where(lane == tok_rows + piece, rounded, out)
        left = left - rounded
    out_ref[...] = out.astype(jnp.bfloat16)


def mix_body(at_ref, routes_ref, filtered_ref, weight_ref, residual_ref, z_ref, out_ref, slot_ref):
    channels = filtered_ref.shape[0]
    tok_rows = z_ref.shape[0]
    experts, capacity, block = out_ref.shape
    expert = lax.broadcasted_iota(jnp.int32, (experts, tok_rows), 0)
    named = [expert == routes_ref[pick : pick + 1] for pick in range(2)]
    earlier = lax.broadcasted_iota(jnp.int32, (tok_rows, tok_rows), 0) < lax.broadcasted_iota(
        jnp.int32, (tok_rows, tok_rows), 1
    )
    rank = jnp.dot(
        jnp.where(named[0] | named[1], 1.0, 0.0).astype(jnp.bfloat16),
        jnp.where(earlier, 1.0, 0.0).astype(jnp.bfloat16),
        preferred_element_type=jnp.float32,
    )
    place = expert.astype(jnp.float32) * capacity + rank
    slots = [
        jnp.sum(jnp.where(who, place, 0.0), 0, keepdims=True).astype(jnp.int32) for who in named
    ]
    slot_ref[:1] = slots[0]
    slot_ref[1:2] = slots[1]

    filtered = filtered_ref[...].astype(jnp.float32)
    gain = jnp.sum(filtered[:, tok_rows : tok_rows + 3], 1, keepdims=True)
    filtered = filtered[:, :tok_rows]
    row_mean = jnp.sum(filtered, 0, keepdims=True) / channels
    row_var = jnp.sum(filtered * filtered, 0, keepdims=True) / channels - row_mean * row_mean
    normed = (filtered - row_mean) * lax.rsqrt(row_var + norm_eps) * gain
    conv_out = (normed * (0.5 + 0.5 * jnp.tanh(0.5 * normed))).astype(jnp.bfloat16)
    mix = lax.dot_general(
        conv_out, weight_ref[...], (((0,), (0,)), ((), ())), preferred_element_type=jnp.float32
    )
    z = residual_alpha * residual_ref[...].astype(jnp.float32) + mix
    z_ref[...] = z
    slot = lax.broadcasted_iota(jnp.int32, (experts * capacity, tok_rows), 0)
    table = (slot == slots[0]) | (slot == slots[1])
    outgoing = jnp.dot(
        jnp.where(table, 1.0, 0.0).astype(jnp.bfloat16),
        z.astype(jnp.bfloat16),
        preferred_element_type=jnp.float32,
    )
    out_ref[...] = outgoing.astype(jnp.bfloat16).reshape(experts, capacity, block)


def down_body(at_ref, mine_ref, else_ref, *refs, picks):
    weights, outs = refs[: 2 * picks], refs[2 * picks :]
    hidden = jnp.concatenate([mine_ref[...], else_ref[...]], 0).T
    down = jnp.concatenate(
        [
            jnp.concatenate([weights[pick][...], weights[picks + pick][...]], 0)
            for pick in range(picks)
        ],
        1,
    )
    part = jnp.dot(hidden, down, preferred_element_type=jnp.float32).astype(jnp.bfloat16)
    groups, _, capacity, block = outs[0].shape
    for number, out_ref in enumerate(outs):
        rows = slice(number * groups * capacity, (number + 1) * groups * capacity)
        for pick in range(picks):
            out_ref[:, pick] = part[rows, pick * block : (pick + 1) * block].reshape(
                groups, capacity, block
            )


def whole(memory=None):
    return pl.BlockSpec(memory_space=memory or pltpu.VMEM)


def full(*shape):
    return pl.BlockSpec(shape, lambda *_: (0,) * len(shape))


def local(
    glu_value,
    glu_gate,
    doc_ids,
    conv_kernel,
    conv_gain,
    out_weight,
    residual,
    mix_gain,
    routes,
    route_weights,
    expert_gate,
    expert_up,
    expert_down,
    final_gain,
):
    f32, bf16 = jnp.float32, jnp.bfloat16
    n_sp, n_yh, n_yl, n_c = (lax.axis_size(axis) for axis in ("sp", "yh", "yl", "c"))
    n_y = n_yh * n_yl
    n_tp = n_y * n_c
    at_tp = lax.axis_index(TP)
    tok_rows, own_ch = glu_value.shape
    features = residual.shape[1]
    feat_block = features // n_tp

    lanes, more = 256, 16
    own_rows, rim = pl.pallas_call(
        head_body,
        out_shape=(
            jax.ShapeDtypeStruct((own_ch + more, lanes), bf16),
            jax.ShapeDtypeStruct((own_ch + more, 128), bf16),
        ),
        in_specs=[whole()] * 3,
        out_specs=(whole(), whole()),
        name="head",
    )(glu_value.T, glu_gate.T, doc_ids[None])
    rim, own_rows, out_weight = lax.optimization_barrier((rim, own_rows, out_weight))
    rim = from_behind(rim, "sp", 1)
    filtered = pl.pallas_call(
        functools.partial(conv_body, lags=conv_kernel.shape[0], tok_rows=tok_rows),
        out_shape=jax.ShapeDtypeStruct((own_ch, lanes), bf16),
        in_specs=[whole()] * 4,
        out_specs=whole(),
        name="conv",
    )(own_rows, rim, conv_kernel, conv_gain[None])
    filtered = lax.all_gather(filtered, TP, axis=0, tiled=True)
    weight_parts = out_weight.reshape(own_ch, n_tp, feat_block).transpose(1, 0, 2)
    weight_own = lax.all_to_all(weight_parts, TP, 0, 0, tiled=True)
    weight_own = weight_own.reshape(-1, feat_block)
    experts = expert_gate.shape[0] * n_sp
    capacity = 4 * tok_rows // experts
    own_z, outgoing, slot_rows = pl.pallas_call(
        mix_body,
        out_shape=(
            jax.ShapeDtypeStruct((tok_rows, feat_block), f32),
            jax.ShapeDtypeStruct((experts, capacity, feat_block), bf16),
            jax.ShapeDtypeStruct((2, tok_rows), jnp.int32),
        ),
        grid_spec=pltpu.PrefetchScalarGridSpec(
            num_scalar_prefetch=1,
            grid=(1,),
            in_specs=[
                full(2, tok_rows),
                full(own_ch * n_tp, lanes),
                full(own_ch * n_tp, feat_block),
                pl.BlockSpec((tok_rows, feat_block), lambda i, at: (0, at[0])),
            ],
            out_specs=(
                full(tok_rows, feat_block),
                full(experts, capacity, feat_block),
                full(2, tok_rows),
            ),
        ),
        name="mix",
    )(at_tp.astype(jnp.int32).reshape(1), routes.T, filtered, weight_own, residual)
    arrived = lax.all_to_all(outgoing, "sp", 0, 0, tiled=True)
    rows = n_sp * capacity
    at_yl, at_c = lax.axis_index("yl"), lax.axis_index("c")
    blocks_send, blocks_keep = (
        ((jnp.arange(n_yh) * n_yl + parity) * n_c + at_c).astype(jnp.int32)
        for parity in (1 - at_yl, at_yl)
    )
    arrived, blocks_send, blocks_keep = lax.optimization_barrier(
        (arrived, blocks_send, blocks_keep)
    )
    arrived = (arrived.reshape(rows, feat_block).T.astype(f32) * row_scale).astype(jnp.float16)
    gathered = lax.all_gather(arrived, TP, axis=0, tiled=True)

    wide = gathered.astype(f32)
    in_mean = jnp.sum(wide, 0) * (1.0 / (row_scale * features))
    in_square = jnp.sum(wide * wide, 0) * (1.0 / (row_scale * row_scale * features))
    in_rstd = lax.rsqrt(in_square - in_mean * in_mean + norm_eps)
    in_rows = (
        (wide * (1.0 / row_scale) - in_mean[None]) * in_rstd[None] * mix_gain[:, None]
    ).astype(bf16)
    gate_proj = jnp.einsum("kf,kr->fr", expert_gate[0], in_rows, preferred_element_type=f32)
    up_proj = jnp.einsum("kf,kr->fr", expert_up[0], in_rows, preferred_element_type=f32)
    hidden = (jax.nn.silu(gate_proj) * up_proj).astype(bf16)

    w_down = expert_down[0]
    units = w_down.shape[0]
    hidden_else, down_else = swap(hidden, "c"), swap(w_down, "c")
    def down(blocks, outs):
        picks = [
            pl.BlockSpec((units, feat_block), lambda i, at, pick=pick: (0, at[pick]))
            for pick in range(n_yh)
        ]
        shape = (n_sp // outs, n_yh, capacity, feat_block)
        return pl.pallas_call(
            functools.partial(down_body, picks=n_yh),
            out_shape=[jax.ShapeDtypeStruct(shape, bf16)] * outs,
            grid_spec=pltpu.PrefetchScalarGridSpec(
                num_scalar_prefetch=1,
                grid=(1,),
                in_specs=[full(units, rows), full(units, rows), *picks, *picks],
                out_specs=[full(*shape)] * outs,
            ),
        )(blocks, hidden, hidden_else, *[w_down] * n_yh, *[down_else] * n_yh)

    near, far = down(blocks_send, 2)
    near = lax.ppermute(near, Y, [(i, i ^ 1) for i in range(n_y)])
    far = lax.ppermute(far, Y, [(i, (i - 1 if i % 2 == 0 else i + 1) % n_y) for i in range(n_y)])
    (kept,) = down(blocks_keep, 1)
    half = n_sp // 2
    parts = kept.at[:half].set((kept[:half].astype(f32) + near.astype(f32)).astype(bf16))
    parts = parts.at[half:].set((parts[half:].astype(f32) + far.astype(f32)).astype(bf16))
    parts = parts.reshape(n_sp * n_yh, capacity, feat_block)
    returned = lax.all_to_all(parts, ("sp", "yh"), 0, 0, tiled=True)
    returned = returned.reshape(experts, n_yh, capacity, feat_block)
    expert_out = jnp.sum(returned.astype(f32), 1).astype(bf16).reshape(rows, feat_block)
    slots = jnp.arange(experts * capacity, dtype=jnp.int32)
    first = (slot_rows[0][:, None] == slots[None, :]).astype(bf16)
    second = (slot_rows[1][:, None] == slots[None, :]).astype(bf16)
    moe_sum = route_weights[:, :1] * jnp.dot(
        first, expert_out, preferred_element_type=f32
    ) + route_weights[:, 1:] * jnp.dot(second, expert_out, preferred_element_type=f32)

    own_gain = lax.dynamic_slice_in_dim(mix_gain, at_tp * feat_block, feat_block, 0)[None]
    z_gain = own_z * own_gain
    sums = jnp.stack(
        [
            jnp.sum(own_z, 1),
            jnp.sum(own_z * own_z, 1),
            jnp.sum(z_gain, 1),
            jnp.sum(z_gain * z_gain, 1),
            jnp.sum(z_gain * own_gain, 1),
            jnp.sum(z_gain * moe_sum, 1),
            jnp.sum(own_gain * moe_sum, 1),
            jnp.sum(moe_sum, 1),
            jnp.sum(moe_sum * moe_sum, 1),
            jnp.zeros_like(moe_sum[:, 0]),
        ]
    )
    sums = summed_over(sums.reshape(-1, 128), TP, n_tp).reshape(10, tok_rows)
    z_mean = sums[0] / features
    z_rstd = lax.rsqrt(sums[1] / features - z_mean * z_mean + norm_eps)
    ar = residual_alpha * z_rstd
    fin_sum = ar * (sums[2] - z_mean * jnp.sum(mix_gain)) + sums[7]
    fin_square = (
        ar * ar * (sums[3] - 2.0 * z_mean * sums[4] + z_mean * z_mean * jnp.sum(mix_gain * mix_gain))
        + 2.0 * ar * (sums[5] - z_mean * sums[6])
        + sums[8]
    )
    fin_mean = fin_sum / features
    fin_rstd = lax.rsqrt(fin_square / features - fin_mean * fin_mean + norm_eps)
    pre_norm = ar[:, None] * (own_z - z_mean[:, None]) * own_gain + moe_sum
    return ((pre_norm - fin_mean[:, None]) * fin_rstd[:, None] * final_gain).astype(bf16)


def solution(mesh):
    finer = Mesh(mesh.devices.reshape(mesh.shape["sp"], 4, 2, 2), ("sp", "yh", "yl", "c"))
    placed = (
        P("sp", TP),
        P("sp", TP),
        P("sp"),
        P(None, TP),
        P(TP),
        P(TP, None),
        P("sp", None),
        P(),
        P("sp", None),
        P("sp", None),
        P("sp", None, TP),
        P("sp", None, TP),
        P("sp", TP, None),
        P(TP),
    )
    return jax.shard_map(
        local, mesh=finer, in_specs=placed, out_specs=P("sp", TP), check_vma=False
    )
```

```python
import functools

import jax
import jax.numpy as jnp
from jax import lax
from jax.experimental import pallas as pl
from jax.experimental.pallas import tpu as pltpu
from jax.sharding import Mesh
from jax.sharding import PartitionSpec as P


Y = ("yh", "yl")
TP = ("yh", "yl", "c")

residual_alpha = 1.41421356
norm_eps = 1e-05
row_scale = 64.0


def from_behind(value, axis, by):
    peers = lax.axis_size(axis)
    pairs = [(i, i + by) for i in range(peers) if 0 <= i + by < peers]
    return lax.ppermute(value, axis, pairs)


def swap(value, axis):
    return lax.ppermute(value, axis, [(0, 1), (1, 0)])


def summed_over(value, axis, peers):
    copies = jnp.broadcast_to(value[None], (peers, *value.shape))
    return jnp.sum(lax.all_to_all(copies, axis, 0, 0, tiled=True), axis=0)


def head_body(value_ref, gate_ref, ids_ref, weight_ref, own_ref, rim_ref, blocks_ref):
    own_ch, tok_rows = value_ref.shape
    gate = gate_ref[...].astype(jnp.float32)
    gated = value_ref[...].astype(jnp.float32) * (1.0 / (1.0 + jnp.exp(-gate)))
    gated = gated.astype(jnp.bfloat16).astype(jnp.float32)
    ids = jnp.broadcast_to(ids_ref[...].astype(jnp.float32), (own_ref.shape[0] - own_ch, tok_rows))
    rows = jnp.concatenate([gated, ids], 0)
    rows = jnp.concatenate([rows, jnp.zeros((rows.shape[0], own_ref.shape[1] - tok_rows), jnp.float32)], 1)
    own_ref[...] = rows.astype(jnp.bfloat16)
    shifted = pltpu.roll(rows, own_ref.shape[1] - (tok_rows - 128), 1)
    rim_ref[...] = shifted[:, :128].astype(jnp.bfloat16)
    block = blocks_ref.shape[2]
    for peer in range(blocks_ref.shape[0]):
        blocks_ref[peer] = weight_ref[:, peer * block : (peer + 1) * block]


def conv_body(own_ref, rim_ref, kernel_ref, gain_ref, out_ref, *, lags, tok_rows):
    own_ch = out_ref.shape[0]
    own = own_ref[...].astype(jnp.float32)
    rim = rim_ref[...].astype(jnp.float32)
    lane = lax.broadcasted_iota(jnp.int32, rim.shape, 1)
    behind = jnp.where(lane < tok_rows - 128, own[:, 128:], rim)
    packed = jnp.concatenate([own[:, :128], behind], 1)
    rows, ids = packed[:own_ch], packed[own_ch : own_ch + 8]
    taps = jnp.concatenate([kernel_ref[...].astype(jnp.float32), gain_ref[...]], 0).T
    total = jnp.zeros_like(rows)
    for lag in range(lags):
        moved = rows if lag == 0 else pltpu.roll(rows, lag, 1)
        other = ids if lag == 0 else pltpu.roll(ids, lag, 1)
        total = total + jnp.where(other[:1] == ids[:1], moved, 0.0) * taps[:, lag : lag + 1]
    left = taps[:, lags : lags + 1]
    lane = lax.broadcasted_iota(jnp.int32, rows.shape, 1)
    out = jnp.where(lane < tok_rows, total, 0.0).astype(jnp.bfloat16).astype(jnp.float32)
    for piece in range(3):
        rounded = left.astype(jnp.bfloat16).astype(jnp.float32)
        out = jnp.where(lane == tok_rows + piece, rounded, out)
        left = left - rounded
    out_ref[...] = out.astype(jnp.bfloat16)


def mix_body(at_ref, routes_ref, filtered_ref, weight_ref, residual_ref, z_ref, out_ref, slot_ref):
    channels = filtered_ref.shape[0]
    tok_rows = z_ref.shape[0]
    experts, capacity, block = out_ref.shape
    expert = lax.broadcasted_iota(jnp.int32, (experts, tok_rows), 0)
    named = [expert == routes_ref[pick : pick + 1] for pick in range(2)]
    earlier = lax.broadcasted_iota(jnp.int32, (tok_rows, tok_rows), 0) < lax.broadcasted_iota(
        jnp.int32, (tok_rows, tok_rows), 1
    )
    rank = jnp.dot(
        jnp.where(named[0] | named[1], 1.0, 0.0).astype(jnp.bfloat16),
        jnp.where(earlier, 1.0, 0.0).astype(jnp.bfloat16),
        preferred_element_type=jnp.float32,
    )
    place = expert.astype(jnp.float32) * capacity + rank
    slots = [
        jnp.sum(jnp.where(who, place, 0.0), 0, keepdims=True).astype(jnp.int32) for who in named
    ]
    slot_ref[:1] = slots[0]
    slot_ref[1:2] = slots[1]

    filtered = filtered_ref[...].astype(jnp.float32)
    gain = jnp.sum(filtered[:, tok_rows : tok_rows + 3], 1, keepdims=True)
    filtered = filtered[:, :tok_rows]
    row_mean = jnp.sum(filtered, 0, keepdims=True) / channels
    row_var = jnp.sum(filtered * filtered, 0, keepdims=True) / channels - row_mean * row_mean
    normed = (filtered - row_mean) * lax.rsqrt(row_var + norm_eps) * gain
    conv_out = (normed * (0.5 + 0.5 * jnp.tanh(0.5 * normed))).astype(jnp.bfloat16)
    mix = lax.dot_general(
        conv_out, weight_ref[...], (((0,), (0,)), ((), ())), preferred_element_type=jnp.float32
    )
    z = residual_alpha * residual_ref[...].astype(jnp.float32) + mix
    z_ref[...] = z
    slot = lax.broadcasted_iota(jnp.int32, (experts * capacity, tok_rows), 0)
    table = (slot == slots[0]) | (slot == slots[1])
    outgoing = jnp.dot(
        jnp.where(table, 1.0, 0.0).astype(jnp.bfloat16),
        z.astype(jnp.bfloat16),
        preferred_element_type=jnp.float32,
    )
    out_ref[...] = outgoing.astype(jnp.bfloat16).reshape(experts, capacity, block)


def down_body(at_ref, hidden_ref, *refs, picks):
    weights, out_ref = refs[: 2 * picks], refs[2 * picks]
    units = weights[0].shape[0]
    first = pl.multiple_of(at_ref[picks] * units, 64)
    second = pl.multiple_of((1 - at_ref[picks]) * units, 64)
    hidden = jnp.concatenate(
        [hidden_ref[pl.ds(first, units)], hidden_ref[pl.ds(second, units)]], 0
    ).T
    down = jnp.concatenate(
        [
            jnp.concatenate([weights[pick][...], weights[picks + pick][...]], 0)
            for pick in range(picks)
        ],
        1,
    )
    part = jnp.dot(hidden, down, preferred_element_type=jnp.float32).astype(jnp.bfloat16)
    groups, _, capacity, block = out_ref.shape
    for pick in range(picks):
        out_ref[:, pick] = part[:, pick * block : (pick + 1) * block].reshape(
            groups, capacity, block
        )


def whole(memory=None):
    return pl.BlockSpec(memory_space=memory or pltpu.VMEM)


def full(*shape):
    return pl.BlockSpec(shape, lambda *_: (0,) * len(shape))


def local(
    glu_value,
    glu_gate,
    doc_ids,
    conv_kernel,
    conv_gain,
    out_weight,
    residual,
    mix_gain,
    routes,
    route_weights,
    expert_gate,
    expert_up,
    expert_down,
    final_gain,
):
    f32, bf16 = jnp.float32, jnp.bfloat16
    n_sp, n_yh, n_yl, n_c = (lax.axis_size(axis) for axis in ("sp", "yh", "yl", "c"))
    n_y = n_yh * n_yl
    n_tp = n_y * n_c
    at_tp = lax.axis_index(TP)
    tok_rows, own_ch = glu_value.shape
    features = residual.shape[1]
    feat_block = features // n_tp

    lanes, more = 256, 16
    own_rows, rim, weight_parts = pl.pallas_call(
        head_body,
        out_shape=(
            jax.ShapeDtypeStruct((own_ch + more, lanes), bf16),
            jax.ShapeDtypeStruct((own_ch + more, 128), bf16),
            jax.ShapeDtypeStruct((n_tp, own_ch, feat_block), bf16),
        ),
        in_specs=[whole()] * 4,
        out_specs=(whole(),) * 3,
        name="head",
    )(glu_value.T, glu_gate.T, doc_ids[None], out_weight)
    rim = from_behind(rim, "sp", 1)
    filtered = pl.pallas_call(
        functools.partial(conv_body, lags=conv_kernel.shape[0], tok_rows=tok_rows),
        out_shape=jax.ShapeDtypeStruct((own_ch, lanes), bf16),
        in_specs=[whole()] * 4,
        out_specs=whole(),
        name="conv",
    )(own_rows, rim, conv_kernel, conv_gain[None])
    filtered = lax.all_gather(filtered, TP, axis=0, tiled=True)
    weight_own = lax.all_to_all(weight_parts, TP, 0, 0, tiled=True)
    weight_own = weight_own.reshape(-1, feat_block)
    experts = expert_gate.shape[0] * n_sp
    capacity = 4 * tok_rows // experts
    own_z, outgoing, slot_rows = pl.pallas_call(
        mix_body,
        out_shape=(
            jax.ShapeDtypeStruct((tok_rows, feat_block), f32),
            jax.ShapeDtypeStruct((experts, capacity, feat_block), bf16),
            jax.ShapeDtypeStruct((2, tok_rows), jnp.int32),
        ),
        grid_spec=pltpu.PrefetchScalarGridSpec(
            num_scalar_prefetch=1,
            grid=(1,),
            in_specs=[
                full(2, tok_rows),
                full(own_ch * n_tp, lanes),
                full(own_ch * n_tp, feat_block),
                pl.BlockSpec((tok_rows, feat_block), lambda i, at: (0, at[0])),
            ],
            out_specs=(
                full(tok_rows, feat_block),
                full(experts, capacity, feat_block),
                full(2, tok_rows),
            ),
        ),
        name="mix",
    )(at_tp.astype(jnp.int32).reshape(1), routes.T, filtered, weight_own, residual)
    arrived = lax.all_to_all(outgoing, "sp", 0, 0, tiled=True)
    rows = n_sp * capacity
    at_yl, at_c = lax.axis_index("yl"), lax.axis_index("c")
    blocks_send, blocks_keep = (
        jnp.append((jnp.arange(n_yh) * n_yl + parity) * n_c + at_c, at_c).astype(jnp.int32)
        for parity in (1 - at_yl, at_yl)
    )
    arrived, blocks_send, blocks_keep = lax.optimization_barrier(
        (arrived, blocks_send, blocks_keep)
    )
    arrived = (arrived.reshape(rows, feat_block).T.astype(f32) * row_scale).astype(jnp.float16)
    gathered = lax.all_gather(arrived, TP, axis=0, tiled=True)

    wide = gathered.astype(f32)
    in_mean = jnp.sum(wide, 0) * (1.0 / (row_scale * features))
    in_square = jnp.sum(wide * wide, 0) * (1.0 / (row_scale * row_scale * features))
    in_rstd = lax.rsqrt(in_square - in_mean * in_mean + norm_eps)
    in_rows = (
        (wide * (1.0 / row_scale) - in_mean[None]) * in_rstd[None] * mix_gain[:, None]
    ).astype(bf16)
    gate_proj = jnp.einsum("kf,kr->fr", expert_gate[0], in_rows, preferred_element_type=f32)
    up_proj = jnp.einsum("kf,kr->fr", expert_up[0], in_rows, preferred_element_type=f32)
    hidden = (jax.nn.silu(gate_proj) * up_proj).astype(bf16)

    w_down = expert_down[0]
    units = w_down.shape[0]
    hidden = lax.all_gather(hidden, "c", axis=0, tiled=True)
    down_else = swap(w_down, "c")
    def down(blocks, share, shares):
        picks = [
            pl.BlockSpec((units, feat_block), lambda i, at, pick=pick: (0, at[pick]))
            for pick in range(n_yh)
        ]
        shape = (n_sp // shares, n_yh, capacity, feat_block)
        return pl.pallas_call(
            functools.partial(down_body, picks=n_yh),
            out_shape=jax.ShapeDtypeStruct(shape, bf16),
            grid_spec=pltpu.PrefetchScalarGridSpec(
                num_scalar_prefetch=1,
                grid=(1,),
                in_specs=[
                    pl.BlockSpec((n_c * units, rows // shares), lambda i, at: (0, share)),
                    *picks,
                    *picks,
                ],
                out_specs=full(*shape),
            ),
        )(blocks, hidden, *[w_down] * n_yh, *[down_else] * n_yh)

    near = down(blocks_send, 0, 2)
    near = lax.ppermute(near, Y, [(i, i ^ 1) for i in range(n_y)])
    far = down(blocks_send, 1, 2)
    far = lax.ppermute(far, Y, [(i, (i - 1 if i % 2 == 0 else i + 1) % n_y) for i in range(n_y)])
    kept = down(blocks_keep, 0, 1)
    half = n_sp // 2
    parts = kept.at[:half].set((kept[:half].astype(f32) + near.astype(f32)).astype(bf16))
    parts = parts.at[half:].set((parts[half:].astype(f32) + far.astype(f32)).astype(bf16))
    parts = parts.reshape(n_sp * n_yh, capacity, feat_block)
    returned = lax.all_to_all(parts, ("sp", "yh"), 0, 0, tiled=True)
    returned = returned.reshape(experts, n_yh, capacity, feat_block)
    expert_out = jnp.sum(returned.astype(f32), 1).astype(bf16).reshape(rows, feat_block)
    slots = jnp.arange(experts * capacity, dtype=jnp.int32)
    first = (slot_rows[0][:, None] == slots[None, :]).astype(bf16)
    second = (slot_rows[1][:, None] == slots[None, :]).astype(bf16)
    moe_sum = route_weights[:, :1] * jnp.dot(
        first, expert_out, preferred_element_type=f32
    ) + route_weights[:, 1:] * jnp.dot(second, expert_out, preferred_element_type=f32)

    own_gain = lax.dynamic_slice_in_dim(mix_gain, at_tp * feat_block, feat_block, 0)[None]
    z_gain = own_z * own_gain
    sums = jnp.stack(
        [
            jnp.sum(own_z, 1),
            jnp.sum(own_z * own_z, 1),
            jnp.sum(z_gain, 1),
            jnp.sum(z_gain * z_gain, 1),
            jnp.sum(z_gain * own_gain, 1),
            jnp.sum(z_gain * moe_sum, 1),
            jnp.sum(own_gain * moe_sum, 1),
            jnp.sum(moe_sum, 1),
            jnp.sum(moe_sum * moe_sum, 1),
            jnp.zeros_like(moe_sum[:, 0]),
        ]
    )
    sums = summed_over(sums.reshape(-1, 128), TP, n_tp).reshape(10, tok_rows)
    z_mean = sums[0] / features
    z_rstd = lax.rsqrt(sums[1] / features - z_mean * z_mean + norm_eps)
    ar = residual_alpha * z_rstd
    fin_sum = ar * (sums[2] - z_mean * jnp.sum(mix_gain)) + sums[7]
    fin_square = (
        ar * ar * (sums[3] - 2.0 * z_mean * sums[4] + z_mean * z_mean * jnp.sum(mix_gain * mix_gain))
        + 2.0 * ar * (sums[5] - z_mean * sums[6])
        + sums[8]
    )
    fin_mean = fin_sum / features
    fin_rstd = lax.rsqrt(fin_square / features - fin_mean * fin_mean + norm_eps)
    pre_norm = ar[:, None] * (own_z - z_mean[:, None]) * own_gain + moe_sum
    return ((pre_norm - fin_mean[:, None]) * fin_rstd[:, None] * final_gain).astype(bf16)


def solution(mesh):
    finer = Mesh(mesh.devices.reshape(mesh.shape["sp"], 4, 2, 2), ("sp", "yh", "yl", "c"))
    placed = (
        P("sp", TP),
        P("sp", TP),
        P("sp"),
        P(None, TP),
        P(TP),
        P(TP, None),
        P("sp", None),
        P(),
        P("sp", None),
        P("sp", None),
        P("sp", None, TP),
        P("sp", None, TP),
        P("sp", TP, None),
        P(TP),
    )
    return jax.shard_map(
        local, mesh=finer, in_specs=placed, out_specs=P("sp", TP), check_vma=False
    )
```

```python
import functools

import jax
import jax.numpy as jnp
from jax import lax
from jax.experimental import pallas as pl
from jax.experimental.pallas import tpu as pltpu
from jax.sharding import Mesh
from jax.sharding import PartitionSpec as P


Y = ("yh", "yl")
TP = ("yh", "yl", "c")

residual_alpha = 1.41421356
norm_eps = 1e-05
row_scale = 64.0


def from_behind(value, axis, by):
    peers = lax.axis_size(axis)
    pairs = [(i, i + by) for i in range(peers) if 0 <= i + by < peers]
    return lax.ppermute(value, axis, pairs)


def swap(value, axis):
    return lax.ppermute(value, axis, [(0, 1), (1, 0)])


def summed_over(value, axis, peers):
    copies = jnp.broadcast_to(value[None], (peers, *value.shape))
    return jnp.sum(lax.all_to_all(copies, axis, 0, 0, tiled=True), axis=0)


def head_body(value_ref, gate_ref, ids_ref, weight_ref, own_ref, rim_ref, blocks_ref):
    own_ch, tok_rows = value_ref.shape
    gate = gate_ref[...].astype(jnp.float32)
    gated = value_ref[...].astype(jnp.float32) * (0.5 + 0.5 * jnp.tanh(0.5 * gate))
    gated = gated.astype(jnp.bfloat16).astype(jnp.float32)
    ids = jnp.broadcast_to(ids_ref[...].astype(jnp.float32), (own_ref.shape[0] - own_ch, tok_rows))
    rows = jnp.concatenate([gated, ids], 0)
    rows = jnp.concatenate([rows, jnp.zeros((rows.shape[0], own_ref.shape[1] - tok_rows), jnp.float32)], 1)
    own_ref[...] = rows.astype(jnp.bfloat16)
    shifted = pltpu.roll(rows, own_ref.shape[1] - (tok_rows - 128), 1)
    rim_ref[...] = shifted[:, :128].astype(jnp.bfloat16)
    block = blocks_ref.shape[2]
    for peer in range(blocks_ref.shape[0]):
        blocks_ref[peer] = weight_ref[:, peer * block : (peer + 1) * block]


def conv_body(own_ref, rim_ref, kernel_ref, gain_ref, out_ref, *, lags, tok_rows):
    own_ch = out_ref.shape[0]
    own = own_ref[...].astype(jnp.float32)
    rim = rim_ref[...].astype(jnp.float32)
    lane = lax.broadcasted_iota(jnp.int32, rim.shape, 1)
    behind = jnp.where(lane < tok_rows - 128, own[:, 128:], rim)
    packed = jnp.concatenate([own[:, :128], behind], 1)
    rows, ids = packed[:own_ch], packed[own_ch : own_ch + 8]
    taps = jnp.concatenate([kernel_ref[...].astype(jnp.float32), gain_ref[...]], 0).T
    total = jnp.zeros_like(rows)
    for lag in range(lags):
        moved = rows if lag == 0 else pltpu.roll(rows, lag, 1)
        other = ids if lag == 0 else pltpu.roll(ids, lag, 1)
        total = total + jnp.where(other[:1] == ids[:1], moved, 0.0) * taps[:, lag : lag + 1]
    left = taps[:, lags : lags + 1]
    lane = lax.broadcasted_iota(jnp.int32, rows.shape, 1)
    out = jnp.where(lane < tok_rows, total, 0.0).astype(jnp.bfloat16).astype(jnp.float32)
    for piece in range(3):
        rounded = left.astype(jnp.bfloat16).astype(jnp.float32)
        out = jnp.where(lane == tok_rows + piece, rounded, out)
        left = left - rounded
    out_ref[...] = out.astype(jnp.bfloat16)


def mix_body(at_ref, routes_ref, filtered_ref, weight_ref, residual_ref, z_ref, out_ref, slot_ref):
    channels = filtered_ref.shape[0]
    tok_rows = z_ref.shape[0]
    experts, capacity, block = out_ref.shape
    expert = lax.broadcasted_iota(jnp.int32, (experts, tok_rows), 0)
    named = [expert == routes_ref[pick : pick + 1] for pick in range(2)]
    earlier = lax.broadcasted_iota(jnp.int32, (tok_rows, tok_rows), 0) < lax.broadcasted_iota(
        jnp.int32, (tok_rows, tok_rows), 1
    )
    rank = jnp.dot(
        jnp.where(named[0] | named[1], 1.0, 0.0).astype(jnp.bfloat16),
        jnp.where(earlier, 1.0, 0.0).astype(jnp.bfloat16),
        preferred_element_type=jnp.float32,
    )
    place = expert.astype(jnp.float32) * capacity + rank
    slots = [
        jnp.sum(jnp.where(who, place, 0.0), 0, keepdims=True).astype(jnp.int32) for who in named
    ]
    slot_ref[:1] = slots[0]
    slot_ref[1:2] = slots[1]

    filtered = filtered_ref[...].astype(jnp.float32)
    gain = jnp.sum(filtered[:, tok_rows : tok_rows + 3], 1, keepdims=True)
    filtered = filtered[:, :tok_rows]
    row_mean = jnp.sum(filtered, 0, keepdims=True) / channels
    row_var = jnp.sum(filtered * filtered, 0, keepdims=True) / channels - row_mean * row_mean
    normed = (filtered - row_mean) * lax.rsqrt(row_var + norm_eps) * gain
    conv_out = (normed * (0.5 + 0.5 * jnp.tanh(0.5 * normed))).astype(jnp.bfloat16)
    mix = lax.dot_general(
        conv_out, weight_ref[...], (((0,), (0,)), ((), ())), preferred_element_type=jnp.float32
    )
    z = residual_alpha * residual_ref[...].astype(jnp.float32) + mix
    z_ref[...] = z
    slot = lax.broadcasted_iota(jnp.int32, (experts * capacity, tok_rows), 0)
    table = (slot == slots[0]) | (slot == slots[1])
    outgoing = jnp.dot(
        jnp.where(table, 1.0, 0.0).astype(jnp.bfloat16),
        z.astype(jnp.bfloat16),
        preferred_element_type=jnp.float32,
    )
    out_ref[...] = outgoing.astype(jnp.bfloat16).reshape(experts, capacity, block)


def down_body(at_ref, hidden_ref, *refs, picks):
    weights, outs = refs[: 2 * picks], refs[2 * picks :]
    units = weights[0].shape[0]
    first = pl.multiple_of(at_ref[picks] * units, 64)
    second = pl.multiple_of((1 - at_ref[picks]) * units, 64)
    hidden = jnp.concatenate(
        [hidden_ref[pl.ds(first, units)], hidden_ref[pl.ds(second, units)]], 0
    ).T
    down = jnp.concatenate(
        [
            jnp.concatenate([weights[pick][...], weights[picks + pick][...]], 0)
            for pick in range(picks)
        ],
        1,
    )
    part = jnp.dot(hidden, down, preferred_element_type=jnp.float32).astype(jnp.bfloat16)
    groups, _, capacity, block = outs[0].shape
    for number, out_ref in enumerate(outs):
        rows = slice(number * groups * capacity, (number + 1) * groups * capacity)
        for pick in range(picks):
            out_ref[:, pick] = part[rows, pick * block : (pick + 1) * block].reshape(
                groups, capacity, block
            )


def whole(memory=None):
    return pl.BlockSpec(memory_space=memory or pltpu.VMEM)


def full(*shape):
    return pl.BlockSpec(shape, lambda *_: (0,) * len(shape))


def local(
    glu_value,
    glu_gate,
    doc_ids,
    conv_kernel,
    conv_gain,
    out_weight,
    residual,
    mix_gain,
    routes,
    route_weights,
    expert_gate,
    expert_up,
    expert_down,
    final_gain,
):
    f32, bf16 = jnp.float32, jnp.bfloat16
    n_sp, n_yh, n_yl, n_c = (lax.axis_size(axis) for axis in ("sp", "yh", "yl", "c"))
    n_y = n_yh * n_yl
    n_tp = n_y * n_c
    at_tp = lax.axis_index(TP)
    tok_rows, own_ch = glu_value.shape
    features = residual.shape[1]
    feat_block = features // n_tp

    lanes, more = 256, 16
    own_rows, rim, weight_parts = pl.pallas_call(
        head_body,
        out_shape=(
            jax.ShapeDtypeStruct((own_ch + more, lanes), bf16),
            jax.ShapeDtypeStruct((own_ch + more, 128), bf16),
            jax.ShapeDtypeStruct((n_tp, own_ch, feat_block), bf16),
        ),
        in_specs=[whole()] * 4,
        out_specs=(whole(),) * 3,
        name="head",
    )(glu_value.T, glu_gate.T, doc_ids[None], out_weight)
    rim = from_behind(rim, "sp", 1)
    filtered = pl.pallas_call(
        functools.partial(conv_body, lags=conv_kernel.shape[0], tok_rows=tok_rows),
        out_shape=jax.ShapeDtypeStruct((own_ch, lanes), bf16),
        in_specs=[whole()] * 4,
        out_specs=whole(),
        name="conv",
    )(own_rows, rim, conv_kernel, conv_gain[None])
    filtered = lax.all_gather(filtered, TP, axis=0, tiled=True)
    weight_own = lax.all_to_all(weight_parts, TP, 0, 0, tiled=True)
    weight_own = weight_own.reshape(-1, feat_block)
    experts = expert_gate.shape[0] * n_sp
    capacity = 4 * tok_rows // experts
    own_z, outgoing, slot_rows = pl.pallas_call(
        mix_body,
        out_shape=(
            jax.ShapeDtypeStruct((tok_rows, feat_block), f32),
            jax.ShapeDtypeStruct((experts, capacity, feat_block), bf16),
            jax.ShapeDtypeStruct((2, tok_rows), jnp.int32),
        ),
        grid_spec=pltpu.PrefetchScalarGridSpec(
            num_scalar_prefetch=1,
            grid=(1,),
            in_specs=[
                full(2, tok_rows),
                full(own_ch * n_tp, lanes),
                full(own_ch * n_tp, feat_block),
                pl.BlockSpec((tok_rows, feat_block), lambda i, at: (0, at[0])),
            ],
            out_specs=(
                full(tok_rows, feat_block),
                full(experts, capacity, feat_block),
                full(2, tok_rows),
            ),
        ),
        name="mix",
    )(at_tp.astype(jnp.int32).reshape(1), routes.T, filtered, weight_own, residual)
    arrived = lax.all_to_all(outgoing, "sp", 0, 0, tiled=True)
    rows = n_sp * capacity
    at_yl, at_c = lax.axis_index("yl"), lax.axis_index("c")
    blocks_send, blocks_keep = (
        jnp.append((jnp.arange(n_yh) * n_yl + parity) * n_c + at_c, at_c).astype(jnp.int32)
        for parity in (1 - at_yl, at_yl)
    )
    arrived, blocks_send, blocks_keep = lax.optimization_barrier(
        (arrived, blocks_send, blocks_keep)
    )
    arrived = (arrived.reshape(rows, feat_block).T.astype(f32) * row_scale).astype(jnp.float16)
    gathered = lax.all_gather(arrived, TP, axis=0, tiled=True)

    wide = gathered.astype(f32)
    in_mean = jnp.sum(wide, 0) * (1.0 / (row_scale * features))
    in_square = jnp.sum(wide * wide, 0) * (1.0 / (row_scale * row_scale * features))
    in_rstd = lax.rsqrt(in_square - in_mean * in_mean + norm_eps)
    in_rows = (
        (wide * (1.0 / row_scale) - in_mean[None]) * in_rstd[None] * mix_gain[:, None]
    ).astype(bf16)
    gate_proj = jnp.einsum("kf,kr->fr", expert_gate[0], in_rows, preferred_element_type=f32)
    up_proj = jnp.einsum("kf,kr->fr", expert_up[0], in_rows, preferred_element_type=f32)
    hidden = (gate_proj * (0.5 + 0.5 * jnp.tanh(0.5 * gate_proj)) * up_proj).astype(bf16)

    w_down = expert_down[0]
    units = w_down.shape[0]
    hidden = lax.all_gather(hidden, "c", axis=0, tiled=True)
    down_else = swap(w_down, "c")
    def down(blocks, outs):
        picks = [
            pl.BlockSpec((units, feat_block), lambda i, at, pick=pick: (0, at[pick]))
            for pick in range(n_yh)
        ]
        shape = (n_sp // outs, n_yh, capacity, feat_block)
        return pl.pallas_call(
            functools.partial(down_body, picks=n_yh),
            out_shape=[jax.ShapeDtypeStruct(shape, bf16)] * outs,
            grid_spec=pltpu.PrefetchScalarGridSpec(
                num_scalar_prefetch=1,
                grid=(1,),
                in_specs=[full(n_c * units, rows), *picks, *picks],
                out_specs=[full(*shape)] * outs,
            ),
        )(blocks, hidden, *[w_down] * n_yh, *[down_else] * n_yh)

    near, far = down(blocks_send, 2)
    near = lax.ppermute(near, Y, [(i, i ^ 1) for i in range(n_y)])
    far = lax.ppermute(far, Y, [(i, (i - 1 if i % 2 == 0 else i + 1) % n_y) for i in range(n_y)])
    (kept,) = down(blocks_keep, 1)
    half = n_sp // 2
    parts = kept.at[:half].set((kept[:half].astype(f32) + near.astype(f32)).astype(bf16))
    parts = parts.at[half:].set((parts[half:].astype(f32) + far.astype(f32)).astype(bf16))
    parts = parts.reshape(n_sp * n_yh, capacity, feat_block)
    returned = lax.all_to_all(parts, ("sp", "yh"), 0, 0, tiled=True)
    returned = returned.reshape(experts, n_yh, capacity, feat_block)
    expert_out = jnp.sum(returned.astype(f32), 1).astype(bf16).reshape(rows, feat_block)
    slots = jnp.arange(experts * capacity, dtype=jnp.int32)
    first = (slot_rows[0][:, None] == slots[None, :]).astype(bf16)
    second = (slot_rows[1][:, None] == slots[None, :]).astype(bf16)
    moe_sum = route_weights[:, :1] * jnp.dot(
        first, expert_out, preferred_element_type=f32
    ) + route_weights[:, 1:] * jnp.dot(second, expert_out, preferred_element_type=f32)

    own_gain = lax.dynamic_slice_in_dim(mix_gain, at_tp * feat_block, feat_block, 0)[None]
    z_gain = own_z * own_gain
    sums = jnp.stack(
        [
            jnp.sum(own_z, 1),
            jnp.sum(own_z * own_z, 1),
            jnp.sum(z_gain, 1),
            jnp.sum(z_gain * z_gain, 1),
            jnp.sum(z_gain * own_gain, 1),
            jnp.sum(z_gain * moe_sum, 1),
            jnp.sum(own_gain * moe_sum, 1),
            jnp.sum(moe_sum, 1),
            jnp.sum(moe_sum * moe_sum, 1),
            jnp.zeros_like(moe_sum[:, 0]),
        ]
    )
    sums = summed_over(sums.reshape(-1, 128), TP, n_tp).reshape(10, tok_rows)
    z_mean = sums[0] / features
    z_rstd = lax.rsqrt(sums[1] / features - z_mean * z_mean + norm_eps)
    ar = residual_alpha * z_rstd
    fin_sum = ar * (sums[2] - z_mean * jnp.sum(mix_gain)) + sums[7]
    fin_square = (
        ar * ar * (sums[3] - 2.0 * z_mean * sums[4] + z_mean * z_mean * jnp.sum(mix_gain * mix_gain))
        + 2.0 * ar * (sums[5] - z_mean * sums[6])
        + sums[8]
    )
    fin_mean = fin_sum / features
    fin_rstd = lax.rsqrt(fin_square / features - fin_mean * fin_mean + norm_eps)
    pre_norm = ar[:, None] * (own_z - z_mean[:, None]) * own_gain + moe_sum
    return ((pre_norm - fin_mean[:, None]) * fin_rstd[:, None] * final_gain).astype(bf16)


def solution(mesh):
    finer = Mesh(mesh.devices.reshape(mesh.shape["sp"], 4, 2, 2), ("sp", "yh", "yl", "c"))
    placed = (
        P("sp", TP),
        P("sp", TP),
        P("sp"),
        P(None, TP),
        P(TP),
        P(TP, None),
        P("sp", None),
        P(),
        P("sp", None),
        P("sp", None),
        P("sp", None, TP),
        P("sp", None, TP),
        P("sp", TP, None),
        P(TP),
    )
    return jax.shard_map(
        local, mesh=finer, in_specs=placed, out_specs=P("sp", TP), check_vma=False
    )
```
